32 devices in a mesh: ep: 16 (over z, y, x), tp: 2 (over core).
Axes of the slice: x: 2, y: 2, z: 4, core: 2. Of those that a mesh axis runs over, the one named last changes fastest.
Arguments:
- inputs: bfloat16 [256, 2048], P('ep'), may hold values from -6 to 6
- positions: int32 [256], P('ep'), may hold values from 1024 to 8191
- ret_state: float32 [256, 12, 128, 128], P('ep', 'tp'), may hold values from -4 to 4
- norm_mix: bfloat16 [2048], replicated, may hold values from 0.099609375 to 1.8984375
- w_query: bfloat16 [2048, 1536], P('ep', 'tp'), may hold values from -0.1875 to 0.1875
- w_key: bfloat16 [2048, 1536], P('ep', 'tp'), may hold values from -0.1875 to 0.1875
- w_value: bfloat16 [2048, 1536], P('ep', 'tp'), may hold values from -0.1875 to 0.1875
- w_gate_in: bfloat16 [2048, 1536], P('ep', 'tp'), may hold values from -0.1875 to 0.1875
- head_gain: bfloat16 [1536], P('tp'), may hold values from 0.099609375 to 1.8984375
- w_out: bfloat16 [1536, 2048], P('tp', 'ep'), may hold values from -0.15625 to 0.15625
- norm_ffn: bfloat16 [2048], replicated, may hold values from 0.099609375 to 1.8984375
- route_ids: int32 [256, 4], P('ep'), may hold values from 0 to 15, all different within a row; in each aligned block of 16 rows (0 to 15, 16 to 31, ...) at most 8 rows name the same one
- route_weight: bfloat16 [256, 4], P('ep'), may hold values from 0.19921875 to 1
- exp_gate: bfloat16 [16, 2048, 1024], P('ep', None, 'tp'), may hold values from -0.125 to 0.125
- exp_up: bfloat16 [16, 2048, 1024], P('ep', None, 'tp'), may hold values from -0.125 to 0.125
- exp_down: bfloat16 [16, 1024, 2048], P('ep', 'tp'), may hold values from -0.1875 to 0.1875
- dense_gate: bfloat16 [2048, 4096], P(None, ('ep', 'tp')), may hold values from -0.125 to 0.125
- dense_up: bfloat16 [2048, 4096], P(None, ('ep', 'tp')), may hold values from -0.125 to 0.125
- dense_down: bfloat16 [4096, 2048], P(('ep', 'tp')), may hold values from -0.1875 to 0.1875
- branch_gate: bfloat16 [2048], replicated, may hold values from -0.125 to 0.125
Outputs:
- layer_out: bfloat16 [256, 2048], P('ep')
- new_state: float32 [256, 12, 128, 128], P('ep', 'tp')
The draws below stay inside these ranges and needn't reach their ends.
Inputs may be any that keep to these rules, and one draw needn't show every extreme that they name: `route_ids`: each row names 4 different experts. Among the rows of one index of ep no expert is named more than 8 times, a bound that some block reaches.
All inputs are finite; a program needn't handle non-finite values.
Results may differ from the reference program's by a relative error of at most 0.015.
Values may be sent and summed in bfloat16 or wider, within the bound.
A program may use at most 128 MiB of HBM per device.

```python
import math
from functools import reduce
import jax
import jax.numpy as jnp
import numpy as np
from jax import lax

D = 2048
HEADS = 12
HEAD_DIM = 128
EXP_FF = 1024
DENSE_FF = 4096
TOP_K = 4
SEQ_DEV = 16
RET_WIDTH = 1536
EXPERTS = 16
TOKENS = 256
CAP = 8
N_EP = 16
N_TP = 2


def place_ends(drawn, stream_key, smallest, top_value):
    index_at = [jax.random.randint(jax.random.fold_in(stream_key, axis), (), 0, length) for axis, length in enumerate(drawn.shape)]
    longest = drawn.shape.index(max(drawn.shape))
    next_to = index_at[:longest] + [(index_at[longest] + 1) % drawn.shape[longest]] + index_at[longest + 1:]
    return drawn.at[tuple(index_at)].set(smallest).at[tuple(next_to)].set(top_value)


def raised(values, own_key, source, target, blocks, factor):
    def block_of(position):
        return (jnp.arange(values.shape[position]) // (values.shape[position] // blocks)).reshape((-1,) + (1,) * (values.ndim - 1 - position))

    first = jax.random.permutation(own_key, blocks)[block_of(target)]
    far = (block_of(target) + blocks // 2) % blocks
    return jnp.where((block_of(source) == first) | (block_of(source) == far), factor * values, values)


def block_scale(key, shape, shards, smallest, top_value):
    def one(axis_at, parts):
        draws = jax.random.uniform(jax.random.fold_in(jax.random.fold_in(key, 6), axis_at), (parts,), jnp.float32, smallest / len(shards), top_value / len(shards))
        return jnp.repeat(jnp.exp(draws), shape[axis_at] // parts).reshape((-1,) + (1,) * (len(shape) - axis_at - 1))

    loudness = one(*shards[0])
    for cut in shards[1:]:
        loudness = loudness * one(*cut)
    return loudness


def deal_out(rng, own, number, rows, amount, top, reach, lean):
    order = jax.random.permutation(rng, amount)
    heavy_load, ordinary = load_shares(amount, rows * top, reach, lean, True), load_shares(amount, rows * top, reach, lean, False)
    places = jnp.arange(amount)

    def named(lengths, turn):
        used = int((lengths > 0).sum())
        fixed = max(1, used // 4)
        moved = fixed + (places - fixed + turn * (used - fixed)) % max(1, amount - fixed)
        return jnp.zeros((amount,), jnp.int32).at[order[jnp.where(places < fixed, places, moved)]].set(jnp.asarray(lengths, jnp.int32))

    lengths = jnp.where(number % 4 == 0, named(heavy_load, number // 4), named(ordinary, number - number // 4 - 1))
    mixed = jax.random.permutation(jax.random.fold_in(own, 3), amount)
    giver, receiver = mixed[0:amount // 2 * 2:2], mixed[1:amount // 2 * 2:2]
    margin = jnp.minimum(lengths[giver] - 1, reach - lengths[receiver]) // 2
    margin = jnp.where((giver == order[0]) | (receiver == order[0]) | (lengths[receiver] == 0), 0, jnp.maximum(margin, 0))
    moved = jax.random.randint(jax.random.fold_in(own, 4), (amount // 2,), 0, 1 << 20) % (margin + 1)
    lengths = lengths.at[giver].add(-moved).at[receiver].add(moved)
    items = jnp.searchsorted(jnp.cumsum(lengths), jnp.arange(rows * top), side="right").astype(jnp.int32)
    grid = items.reshape(top, rows).T
    grid = grid[jax.random.permutation(jax.random.fold_in(own, 1), rows)]
    turn = jax.random.randint(jax.random.fold_in(own, 2), (rows, 1), 0, top)
    return jnp.take_along_axis(grid, (jnp.arange(top)[None, :] + turn) % top, axis=1)


def load_shares(amount, total, bound, slope, full):
    portions = [(1 << 20) // math.isqrt(standing ** slope) + 1 for standing in range(1, amount + 1)]
    largest = bound if full else min(bound, max(-(-total // amount), total * portions[0] // sum(portions)))
    least = 1 if total - largest >= amount - 1 else 0
    given, rest = [largest] + [least] * (amount - 1), total - largest - least * (amount - 1)
    while rest > 0:
        candidates = [i for i in range(1, amount) if given[i] < largest] or [i for i in range(1, amount) if given[i] < bound]
        pool, budget = sum([portions[i] for i in candidates]), rest
        for i in candidates:
            addition = min(bound - given[i], max(1, budget * portions[i] // pool), rest)
            given[i] = given[i] + addition
            rest = rest - addition
    return np.array(given)


def scatter_about(stream_key, dims, scale, bound, pieces=(), kind=jnp.bfloat16):
    drawn = jax.random.normal(stream_key, dims, jnp.float32) * scale
    if len(pieces) > 0:
        drawn = block_scale(stream_key, dims, pieces, -0.22, 0.18) * drawn
    return jnp.clip(drawn, min=-bound, max=bound).astype(kind)


def gaussian_with(key, dims, deviation, reach, shards, heavy, kind=jnp.bfloat16):
    values = deviation * jax.random.normal(key, dims, jnp.float32)
    if shards:
        values = values * block_scale(key, dims, shards, -0.22, 0.18)
    return jnp.clip(raised(values, jax.random.fold_in(key, 3), *heavy), -reach, reach).astype(kind)


def setup_inputs(seed: int = 0) -> dict:
    keys = jax.random.split(jax.random.key(seed), 21)
    inputs = scatter_about(keys[0], (TOKENS, D), 1.0, 6.0, ((0, 16),))
    positions = place_ends(jax.random.randint(keys[1], (TOKENS,), 1024, 8192), jax.random.fold_in(keys[1], 1), 1024, 8191).astype(jnp.int32)
    ret_state = scatter_about(keys[2], (TOKENS, HEADS, HEAD_DIM, HEAD_DIM), 0.25, 4.0, ((0, 16), (1, 2)), jnp.float32)
    norm_mix = jnp.clip(1.0 + 0.18 * jax.random.normal(keys[3], (D,), jnp.float32), 0.099609375, 1.8984375).astype(jnp.bfloat16)
    w_query = gaussian_with(keys[4], (D, RET_WIDTH), D ** -0.5, 0.1875, ((0, 16), (1, 2)), (0, 1, 16, 2.0))
    w_key = gaussian_with(keys[5], (D, RET_WIDTH), D ** -0.5, 0.1875, ((0, 16), (1, 2)), (0, 1, 16, 2.0))
    w_value = gaussian_with(keys[6], (D, RET_WIDTH), D ** -0.5, 0.1875, ((0, 16), (1, 2)), (0, 1, 16, 2.0))
    w_gate_in = gaussian_with(keys[7], (D, RET_WIDTH), D ** -0.5, 0.1875, ((0, 16), (1, 2)), (0, 1, 16, 2.0))
    head_gain = jnp.clip(1.0 + 0.18 * jax.random.normal(keys[8], (RET_WIDTH,), jnp.float32), 0.099609375, 1.8984375).astype(jnp.bfloat16)
    w_out = scatter_about(keys[9], (RET_WIDTH, D), RET_WIDTH ** -0.5, 0.15625, ((0, 2), (1, 16)))
    norm_ffn = jnp.clip(1.0 + 0.18 * jax.random.normal(keys[10], (D,), jnp.float32), 0.099609375, 1.8984375).astype(jnp.bfloat16)
    route_ids_keys = jax.random.split(jax.random.fold_in(keys[11], 1), TOKENS // SEQ_DEV)
    route_ids_turns = jax.random.permutation(jax.random.fold_in(keys[11], 3), TOKENS // SEQ_DEV)
    route_ids = jax.vmap(lambda own, number: deal_out(jax.random.fold_in(keys[11], 2), own, number, SEQ_DEV, EXPERTS, TOP_K, CAP, 2))(route_ids_keys, route_ids_turns).reshape((TOKENS, TOP_K))
    route_weight = jnp.clip(jnp.exp(math.log(1.0) - 1.6133518 * jax.random.uniform(keys[12], (TOKENS, TOP_K), jnp.float32) ** block_scale(keys[12], (TOKENS, TOP_K), ((0, 16),), -0.2, 0.2)), 0.19921875, 1.0).astype(jnp.bfloat16)
    exp_gate = scatter_about(keys[13], (EXPERTS, D, EXP_FF), D ** -0.5, 0.125, ((0, 16), (2, 2)))
    exp_up = scatter_about(keys[14], (EXPERTS, D, EXP_FF), D ** -0.5, 0.125, ((0, 16), (2, 2)))
    exp_down = scatter_about(keys[15], (EXPERTS, EXP_FF, D), EXP_FF ** -0.5, 0.1875, ((0, 16), (1, 2)))
    dense_gate = scatter_about(keys[16], (D, DENSE_FF), D ** -0.5, 0.125, ((1, 32),))
    dense_up = scatter_about(keys[17], (D, DENSE_FF), D ** -0.5, 0.125, ((1, 32),))
    dense_down = gaussian_with(keys[18], (DENSE_FF, D), DENSE_FF ** -0.5, 0.1875, ((0, 32),), (0, 1, 32, 2.75))
    branch_gate = scatter_about(keys[19], (D,), D ** -0.5, 0.125)
    return {"inputs": inputs, "positions": positions, "ret_state": ret_state, "norm_mix": norm_mix, "w_query": w_query, "w_key": w_key, "w_value": w_value, "w_gate_in": w_gate_in, "head_gain": head_gain, "w_out": w_out, "norm_ffn": norm_ffn, "route_ids": route_ids, "route_weight": route_weight, "exp_gate": exp_gate, "exp_up": exp_up, "exp_down": exp_down, "dense_gate": dense_gate, "dense_up": dense_up, "dense_down": dense_down, "branch_gate": branch_gate}


EPS = 1e-06

def rms_scale(values, scales):
    widened = values.astype(jnp.float32)
    scaled = widened * lax.rsqrt(lax.optimization_barrier(jnp.mean(widened * widened, axis=-1, keepdims=True)) + EPS)
    return (scaled * scales.astype(jnp.float32)).astype(jnp.bfloat16)

def rotary_angles(positions, head_dim):
    halfway = head_dim // 2
    frequency = 10000.0 ** (-jnp.arange(halfway, dtype=jnp.float32) * 2.0 / head_dim)
    return positions.astype(jnp.float32)[:, None] * frequency[None, :]

def rotate_heads(values, angles):
    halfway = values.shape[-1] // 2
    cosine = jnp.cos(angles)[:, None, :]
    sine_of = jnp.sin(angles)[:, None, :]
    leading = values[..., :halfway]
    trailing = values[..., halfway:]
    return jnp.concatenate([leading * cosine - trailing * sine_of, trailing * cosine + leading * sine_of], axis=-1)

def log_decay(head_count):
    spread = jnp.arange(head_count, dtype=jnp.float32) * (5.0 / max(head_count - 1, 1))
    return jnp.log1p(-2.0 ** (-5.0 - spread))

def retain(queries, keys_in, values_in, gate_pre, old_state, positions, scales, log_gamma):
    row_count, head_count, head_dim = (old_state.shape[0], old_state.shape[1], old_state.shape[2])
    angles = rotary_angles(positions, head_dim)
    rot_query = rotate_heads(queries.astype(jnp.float32).reshape(row_count, head_count, head_dim), angles)
    rot_key = rotate_heads(keys_in.astype(jnp.float32).reshape(row_count, head_count, head_dim), angles) * head_dim ** (-0.5)
    value_heads = values_in.astype(jnp.float32).reshape(row_count, head_count, head_dim)
    new_state = jnp.exp(log_gamma)[None, :, None, None] * old_state + rot_key[:, :, :, None] * value_heads[:, :, None, :]
    readout = jnp.einsum('shd,shdv->shv', rot_query, new_state, precision=lax.Precision.HIGHEST)
    centred = readout - lax.optimization_barrier(jnp.mean(readout, axis=-1, keepdims=True))
    normed = centred * lax.rsqrt(lax.optimization_barrier(jnp.mean(centred * centred, axis=-1, keepdims=True)) + EPS)
    normed = normed * scales.astype(jnp.float32).reshape(head_count, head_dim)
    gated_out = normed.reshape(row_count, head_count * head_dim) * jax.nn.silu(gate_pre.astype(jnp.float32))
    return (gated_out.astype(jnp.bfloat16), new_state)

def expert_total(normed_ffn, route_ids, route_share, exp_gate, exp_up, exp_down):
    token_count = normed_ffn.shape[0]
    flat_ids = route_ids.reshape(-1)
    flat_share = route_share.reshape(-1)
    most_rows = N_EP * CAP

    def one_expert(running, expert):
        matches = flat_ids == expert
        where_hit = jnp.nonzero(matches, size=most_rows, fill_value=0)[0].astype(jnp.int32)
        in_use = jnp.arange(most_rows, dtype=jnp.int32) < jnp.sum(matches.astype(jnp.int32))
        token_of = (where_hit // TOP_K).astype(jnp.int32)
        chosen = normed_ffn[token_of]
        gate_part = jnp.dot(chosen, exp_gate[expert], preferred_element_type=jnp.float32)
        up_part = jnp.dot(chosen, exp_up[expert], preferred_element_type=jnp.float32)
        hidden = (jax.nn.silu(gate_part) * up_part).astype(jnp.bfloat16)
        result = jnp.dot(hidden, exp_down[expert], preferred_element_type=jnp.float32)
        picked = flat_share[where_hit]
        weight = jnp.where(in_use, picked, jnp.zeros_like(picked))
        return (running.at[token_of].add(result * weight[:, None]), None)
    running, _ = lax.scan(one_expert, jnp.zeros((token_count, D), jnp.float32), jnp.arange(EXPERTS, dtype=jnp.int32))
    return running

def reference(inputs, positions, ret_state, norm_mix, w_query, w_key, w_value, w_gate_in, head_gain, w_out, norm_ffn, route_ids, route_weight, exp_gate, exp_up, exp_down, dense_gate, dense_up, dense_down, branch_gate):
    normed = rms_scale(inputs, norm_mix)
    queries = jnp.dot(normed, w_query, preferred_element_type=jnp.float32).astype(jnp.bfloat16)
    keys_new = jnp.dot(normed, w_key, preferred_element_type=jnp.float32).astype(jnp.bfloat16)
    values_new = jnp.dot(normed, w_value, preferred_element_type=jnp.float32).astype(jnp.bfloat16)
    gate_pre = jnp.dot(normed, w_gate_in, preferred_element_type=jnp.float32).astype(jnp.bfloat16)
    retained, new_state = retain(queries, keys_new, values_new, gate_pre, ret_state, positions, head_gain, log_decay(HEADS))
    group_width = RET_WIDTH // N_TP
    halves = [lax.optimization_barrier(jnp.dot(retained[:, member * group_width:(member + 1) * group_width], w_out[member * group_width:(member + 1) * group_width], preferred_element_type=jnp.float32).astype(jnp.bfloat16)).astype(jnp.float32) for member in range(N_TP)]
    mixer_out = reduce(jnp.add, halves).astype(jnp.bfloat16)
    residual_sum = (inputs.astype(jnp.float32) + mixer_out.astype(jnp.float32)).astype(jnp.bfloat16)
    normed_ffn = rms_scale(residual_sum, norm_ffn)
    dense_hidden = (jax.nn.silu(jnp.dot(normed_ffn, dense_gate, preferred_element_type=jnp.float32)) * jnp.dot(normed_ffn, dense_up, preferred_element_type=jnp.float32)).astype(jnp.bfloat16)
    dense_result = jnp.dot(dense_hidden, dense_down, preferred_element_type=jnp.float32)
    branch_open = jax.nn.sigmoid(jnp.dot(normed_ffn, branch_gate[:, None], preferred_element_type=jnp.float32))
    widened = route_weight.astype(jnp.float32)
    route_share = widened / lax.optimization_barrier(jnp.sum(widened, axis=-1, keepdims=True))
    experts_out = expert_total(normed_ffn, route_ids, route_share, exp_gate, exp_up, exp_down)
    layer_out = (residual_sum.astype(jnp.float32) + experts_out + branch_open * dense_result).astype(jnp.bfloat16)
    return (layer_out, new_state)
```

```python
import functools
import math

import jax
import jax.numpy as jnp
import numpy as np
from jax import lax
from jax.experimental import pallas as pl
from jax.experimental.pallas import tpu as pltpu
from jax.sharding import PartitionSpec as P

HEADS = 12
EPS = 1e-06
MESH = pl.DeviceIdType.MESH
LANES = 128
F32 = jnp.float32
BF16 = jnp.bfloat16
INNER = 4
CHUNKS = 2


def decay(head, head_count):
    return 1.0 - 2.0 ** (-5.0 - 5.0 * head / max(head_count - 1, 1))


def normalize(values, gain):
    return (values * lax.rsqrt(jnp.mean(values * values, axis=-1, keepdims=True) + EPS) * gain).astype(
        BF16
    )


def remote(src, dst, send, recv, ep, tp):
    return pltpu.make_async_remote_copy(
        src_ref=src,
        dst_ref=dst,
        send_sem=send,
        recv_sem=recv,
        device_id=(ep, tp),
        device_id_type=MESH,
    )


def layer_kernel(
    n, heads, dim,
    x_hbm, pos_hbm, freq_hbm, ids_hbm, weight_hbm, nmix_hbm, nffn_hbm, open_hbm, gain_hbm,
    state_hbm, wq, wk, wv, wg, wout_hbm, eg_hbm, eu_hbm, ed_hbm, dg_hbm, du_hbm, dd_hbm,
    out_ref, key_ref, value_ref,
    x_ref, pos_ref, freq_ref, ids_ref, weight_ref, nmix_ref, nffn_ref, open_ref, gain_ref,
    state, eg, eu, ed, dg, du, dd,
    xsend, xrows, wcol, wo, wo_flat, parts, zin, zsum, qkvg,
    gain_wide, table, share_out, shares, cos_ref, sin_ref, readout, kept, heads_in,
    mixs, mixin, row, half_out, gathered, open_rows, acc, hidden, dense_hidden, opening,
    other, other_in, summed, plane_in, line_out, line_in, final, final_in,
    load, xs, xr, ws, wr, local, outs, outr, shs, shr, zs, zr, ps, pr, cs, cr, ds, dr,
    ezs, eps, er, ms, mr, sws, swr, f1s, f1r, f2s, f2r, fs, fr,
):
    me, tp = lax.axis_index("ep"), lax.axis_index("tp")
    mate = 1 - tp
    outer = n // INNER
    span = outer // 2
    o, i = me // INNER, lax.rem(me, INNER)
    seqs, width = x_ref.shape
    block, half, tokens, group = width // n, width // 2, n * seqs, INNER * seqs
    kb = INNER * block
    hw = heads * dim

    small = [
        pltpu.make_async_copy(src, dst, load.at[j])
        for j, (src, dst) in enumerate(
            ((x_hbm, x_ref), (nmix_hbm, nmix_ref), (ids_hbm, ids_ref), (weight_hbm, weight_ref),
             (pos_hbm, pos_ref), (freq_hbm, freq_ref), (nffn_hbm, nffn_ref), (open_hbm, open_ref),
             (gain_hbm, gain_ref))
        )
    ]
    large = [
        pltpu.make_async_copy(src, dst, load.at[len(small) + j])
        for j, (src, dst) in enumerate(
            ((state_hbm, state), (eg_hbm.at[0], eg), (eu_hbm.at[0], eu), (dg_hbm, dg),
             (du_hbm, du), (ed_hbm.at[0], ed), (dd_hbm, dd))
        )
    ]
    for copy in small:
        copy.start()

    barrier = pltpu.get_barrier_semaphore()

    def greet(ep, core):
        pl.semaphore_signal(barrier, inc=1, device_id=(ep, core), device_id_type=MESH)

    @pl.loop(1, n)
    def _(k):
        greet(lax.rem(me + k, n), tp)

    for j in range(INNER):
        greet(o * INNER + j, mate)

    @pl.loop(1, outer)
    def _(k):
        greet(lax.rem(o + k, outer) * INNER + i, mate)

    small[0].wait()
    small[1].wait()
    normed = normalize(x_ref[...].astype(F32), nmix_ref[...].astype(F32).reshape(1, width))
    for z in range(outer):
        xsend[z] = normed[:, z * kb : (z + 1) * kb]
    pl.semaphore_wait(barrier, n - 1 + INNER + outer - 1)

    @pl.loop(1, n)
    def _(k):
        peer = lax.rem(me + k, n)
        remote(xsend.at[peer // INNER], xrows.at[me], xs.at[k], xr.at[k], peer, tp).start()

    for m, w in enumerate((wq, wk, wv, wg)):
        own_block = pltpu.make_async_copy(w, wcol.at[i], local.at[0])

        @pl.when(i != m)
        def _(m=m, w=w):
            remote(w, wcol.at[i], ws.at[m], wr.at[i], o * INNER + m, tp).start()

        @pl.when(i == m)
        def _(own_block=own_block):
            own_block.start()

    for copy in large:
        copy.start()
    xrows[me] = xsend[o]

    for j in (2, 3, 4, 5, 6, 7, 8):
        small[j].wait()
    widened = weight_ref[...].astype(F32)
    part = widened / jnp.sum(widened, axis=0, keepdims=True)
    expert = lax.broadcasted_iota(jnp.int32, (n, seqs), 0)
    named = jnp.zeros((n, seqs), F32)
    for j in range(ids_ref.shape[0]):
        named = named + jnp.where(ids_ref[j : j + 1, :] == expert, part[j : j + 1, :], 0.0)
    table[...] = jnp.zeros_like(table)
    table[:n, :seqs] = named
    share_out[...] = table[...].T[:seqs]

    @pl.loop(1, n)
    def _(k):
        peer = lax.rem(me + k, n)
        remote(share_out, shares.at[me], shs.at[k], shr.at[k], peer, tp).start()

    shares[me] = share_out[...]

    rows_at = lax.broadcasted_iota(jnp.int32, (seqs, dim), 0)
    place = jnp.zeros((seqs, dim), F32)
    for s in range(seqs):
        place = jnp.where(rows_at == s, pos_ref[s].astype(F32), place)
    angles = place * freq_ref[...]
    lower = lax.broadcasted_iota(jnp.int32, (seqs, dim), 1) < dim // 2
    cos_ref[...] = jnp.cos(angles)
    sine = jnp.sin(angles)
    sin_ref[...] = jnp.where(lower, -sine, sine)
    open_rows[...] = jnp.broadcast_to(open_ref[...].astype(F32).reshape(1, width), open_rows.shape).astype(BF16)

    gain_wide[...] = gain_ref[...].astype(F32).reshape(1, hw)

    @pl.loop(1, n)
    def _(k):
        peer, came = lax.rem(me + k, n), lax.rem(me + n - k, n)
        copy = remote(xsend.at[peer // INNER], xrows.at[came], xs.at[k], xr.at[k], peer, tp)
        copy.wait_send()
        copy.wait_recv()

    for m, w in enumerate((wq, wk, wv, wg)):
        copy = remote(w, wcol.at[m], ws.at[m], wr.at[m], o * INNER + m, tp)

        @pl.when(i != m)
        def _(copy=copy):
            copy.wait_send()
            copy.wait_recv()

        @pl.when(i == m)
        def _(m=m, w=w):
            pltpu.make_async_copy(w, wcol.at[m], local.at[0]).wait()

    product = jnp.dot(
        xrows[...].reshape(tokens, block * INNER),
        wcol[...].reshape(kb, hw),
        preferred_element_type=F32,
    )
    parts[...] = product.astype(BF16).reshape(outer, group, hw)

    def to_line(k, source):
        peer = lax.rem(o + k, outer)
        return remote(parts.at[peer], zin.at[source], zs.at[k], zr.at[k], peer * INNER + i, tp)

    @pl.loop(1, outer)
    def _(k):
        to_line(k, o).start()

    holder, slot = o // span, lax.rem(o, span)

    @pl.loop(1, outer)
    def _(k):
        peer = lax.rem(o + k, outer)
        remote(
            wout_hbm, wo.at[tp, slot], outs.at[k], outr.at[tp, slot], peer * INNER + i, holder
        ).start()

    @pl.when(holder == tp)
    def _():
        pltpu.make_async_copy(wout_hbm, wo.at[tp, slot], local.at[1]).start()

    @pl.when(holder != tp)
    def _():
        remote(wout_hbm, wo.at[tp, slot], outs.at[0], outr.at[tp, slot], me, mate).start()

    @pl.loop(1, outer)
    def _(k):
        copy = to_line(k, lax.rem(o + outer - k, outer))
        copy.wait_send()
        copy.wait_recv()

    zin[o] = parts[o]
    total = lax.fori_loop(
        0, outer, lambda z, carry: carry + zin[z].astype(F32), jnp.zeros((group, hw), F32)
    )
    zsum[...] = total.astype(BF16).reshape(INNER, seqs, hw)

    def to_plane(k, source):
        peer = lax.rem(i + k, INNER)
        return remote(zsum.at[peer], qkvg.at[source], ps.at[k], pr.at[k], o * INNER + peer, tp)

    for k in range(1, INNER):
        to_plane(k, i).start()
    qkvg[i] = zsum[i]
    large[0].wait()
    for k in range(1, INNER):
        copy = to_plane(k, lax.rem(i + INNER - k, INNER))
        copy.wait_send()
        copy.wait_recv()

    def head(h, carry):
        at = pl.ds(pl.multiple_of(h * dim, dim), dim)
        gamma = F32(0.0)
        for j in range(heads):
            low, high = decay(j, HEADS), decay(heads + j, HEADS)
            gamma = jnp.where(h == j, jnp.where(tp == 0, F32(low), F32(high)), gamma)

        def rotated(ref):
            val = ref[:, at].astype(F32)
            return val * cos_ref[...] + pltpu.roll(val, dim // 2, 1) * sin_ref[...]

        query = rotated(qkvg.at[0])
        key = rotated(qkvg.at[1]) * dim ** (-0.5)
        key_ref[:, at] = key
        value = qkvg[2, :, at].astype(F32)
        across = query.T
        for s in range(seqs):
            readout[s : s + 1, :] = jnp.sum(
                state[s, h] * across[:, s : s + 1], axis=0, keepdims=True
            )
        read = gamma * readout[...] + jnp.sum(query * key, axis=-1, keepdims=True) * value
        centred = read - jnp.mean(read, axis=-1, keepdims=True)
        scaled = centred * lax.rsqrt(jnp.mean(centred * centred, axis=-1, keepdims=True) + EPS)
        gate = qkvg[3, :, at].astype(F32)
        gain = gain_wide[:, at]
        kept[:, at] = (scaled * gain * (gate * jax.nn.sigmoid(gate))).astype(BF16)
        return carry

    lax.fori_loop(0, heads, head, 0)
    value_ref[...] = qkvg[2]

    mine = tp * INNER + i

    def to_group(src, dst, send, recv, j):
        core = lax.rem(tp + j // INNER, 2)
        peer = lax.rem(i + j % INNER, INNER)
        return remote(src(peer), dst, send.at[j], recv.at[j], o * INNER + peer, core)

    def source_of(j):
        core = lax.rem(tp + 2 - j // INNER, 2)
        return core * INNER + lax.rem(i + INNER - j % INNER, INNER)

    ring = (1, 2, 3, 4, 5, 6, 7)
    for j in ring:
        to_group(lambda p: kept, heads_in.at[mine], cs, cr, j).start()
    heads_in[mine] = kept[...]

    @pl.loop(1, outer)
    def _(k):
        peer = lax.rem(o + k, outer)
        remote(
            wout_hbm, wo.at[tp, slot], outs.at[k], outr.at[tp, slot], peer * INNER + i, holder
        ).wait_send()

    @pl.when(holder == tp)
    def _():
        pltpu.make_async_copy(wout_hbm, wo.at[tp, slot], local.at[1]).wait()

    @pl.when(holder != tp)
    def _():
        remote(wout_hbm, wo.at[tp, slot], outs.at[0], outr.at[tp, slot], me, mate).wait_send()

    for core in range(2):
        for s in range(span):

            @pl.when(jnp.logical_not(jnp.logical_and(core == tp, tp * span + s == o)))
            def _(core=core, s=s):
                remote(
                    wout_hbm, wo.at[core, s], outs.at[0], outr.at[core, s], me, mate
                ).wait_recv()

            wo_flat[core, :, s * block : (s + 1) * block] = wo[core, s]

    for j in ring:
        copy = to_group(lambda p: kept, heads_in.at[source_of(j)], cs, cr, j)
        copy.wait_send()
        copy.wait_recv()

    first, second = (
        jnp.dot(
            heads_in[c * INNER : (c + 1) * INNER].reshape(group, hw),
            wo_flat[c],
            preferred_element_type=F32,
        ).astype(BF16)
        for c in range(2)
    )
    mixs[...] = (first.astype(F32) + second.astype(F32)).astype(BF16).reshape(
        INNER, seqs, span * block
    )
    for j in ring:
        to_group(lambda p: mixs.at[p], mixin.at[mine], ds, dr, j).start()
    mixin[mine] = mixs[i]
    for j in ring:
        copy = to_group(lambda p: mixs.at[p], mixin.at[source_of(j)], ds, dr, j)
        copy.wait_send()
        copy.wait_recv()

    for z in range(outer):
        for j in range(INNER):
            b = z * INNER + j
            row[:, b * block : (b + 1) * block] = mixin[
                (z // span) * INNER + j, :, (z % span) * block : (z % span + 1) * block
            ].astype(F32)
    residual = (x_ref[...].astype(F32) + row[...]).astype(BF16).astype(F32)
    row[...] = residual
    normed = normalize(residual, nffn_ref[...].astype(F32).reshape(1, width))
    for c in range(2):
        half_out[c] = normed[:, c * half : (c + 1) * half]

    def along(k, block_id):
        peer = lax.rem(o + k, outer)
        return remote(
            half_out.at[tp], gathered.at[tp, block_id], ezs.at[k], er.at[block_id],
            peer * INNER + i, tp,
        )

    def inside(src, k, z, block_id):
        peer = lax.rem(i + k, INNER)
        return remote(
            src, gathered.at[tp, block_id], eps.at[z, k], er.at[block_id], o * INNER + peer, tp
        )

    def across_cores(half_id, block_id, k):
        return remote(
            gathered.at[tp, block_id], gathered.at[half_id, block_id], ms.at[k], mr.at[k], me, mate
        )

    @pl.loop(1, outer)
    def _(k):
        along(outer - k, me).start()

    for k in range(1, INNER):
        inside(half_out.at[tp], k, 0, me).start()
    for c in range(2):
        gathered[c, me] = half_out[c]

    def block_of(kz, ki):
        return lax.rem(o + outer - kz, outer) * INNER + lax.rem(i + INNER - ki, INNER)

    @pl.loop(1, outer)
    def _(k):
        came = block_of(k, 0)
        along(k, came).wait_recv()
        for j in range(1, INNER):
            inside(gathered.at[tp, came], j, k, came).start()
        across_cores(tp, came, k * INNER).start()

    @pl.loop(0, outer)
    def _(k):
        for j in range(1, INNER):
            came = block_of(k, j)
            inside(half_out.at[tp], j, k, came).wait_recv()
            across_cores(tp, came, k * INNER + j).start()

    for copy in large[1:]:
        copy.wait()

    cols = eg.shape[1]
    dcols = dg.shape[1]
    tile = min(256, cols)
    wide = 2 * cols

    def half_dot(c, first):
        left = gathered[c].reshape(tokens, half)
        k_at = pl.ds(pl.multiple_of(c * half, half), half)

        def put(at, value):
            if first:
                acc[:, at] = value
            else:
                acc[:, at] += value

        for base, w in ((0, eg), (cols, eu)):

            @pl.loop(0, cols // tile)
            def _(j, base=base, w=w):
                src = pl.ds(pl.multiple_of(j * tile, tile), tile)
                dst = pl.ds(pl.multiple_of(base + j * tile, tile), tile)
                put(dst, jnp.dot(left, w[k_at, src], preferred_element_type=F32))

        for base, w in ((wide, dg), (wide + dcols, du)):
            put(slice(base, base + dcols), jnp.dot(left, w[k_at, :], preferred_element_type=F32))
        put(
            slice(wide + 2 * dcols, wide + 2 * dcols + LANES),
            lax.dot_general(
                left, open_rows[:, k_at], (((1,), (1,)), ((), ())), preferred_element_type=F32
            ),
        )

    half_dot(tp, True)

    @pl.loop(1, n)
    def _(q):
        k, j = q // INNER, lax.rem(q, INNER)
        copy = across_cores(mate, block_of(k, j), q)
        copy.wait_send()
        copy.wait_recv()

    half_dot(mate, False)

    @pl.loop(1, outer)
    def _(k):
        along(k, me).wait_send()

    @pl.loop(0, outer)
    def _(k):
        for j in range(1, INNER):
            inside(half_out.at[tp], j, k, me).wait_send()

    @pl.loop(1, n)
    def _(k):
        peer, came = lax.rem(me + k, n), lax.rem(me + n - k, n)
        copy = remote(share_out, shares.at[came], shs.at[k], shr.at[k], peer, tp)
        copy.wait_send()
        copy.wait_recv()

    lane = lax.broadcasted_iota(jnp.int32, (tokens, LANES), 1)
    opening[:, :LANES] = jnp.broadcast_to(
        jnp.sum(
            jnp.where(lane == me, shares[...].reshape(tokens, LANES), 0.0), axis=-1, keepdims=True
        ),
        (tokens, LANES),
    )
    opening[:, LANES:] = jax.nn.sigmoid(acc[:, wide + 2 * dcols : wide + 2 * dcols + LANES])

    @pl.loop(0, cols // tile)
    def _(j):
        at = pl.ds(pl.multiple_of(j * tile, tile), tile)
        gate, up = acc[:, at], acc[:, pl.ds(pl.multiple_of(cols + j * tile, tile), tile)]
        hidden[:, at] = (gate * jax.nn.sigmoid(gate) * up).astype(BF16)

    gate = acc[:, wide : wide + dcols]
    dense_hidden[...] = (
        gate * jax.nn.sigmoid(gate) * acc[:, wide + dcols : wide + 2 * dcols]
    ).astype(BF16)

    piece = half // CHUNKS
    step = min(256, piece)

    def branch(at):
        expert_part = jnp.dot(hidden[...], ed[:, at], preferred_element_type=F32)
        dense_part = jnp.dot(dense_hidden[...], dd[:, at], preferred_element_type=F32)
        return expert_part * opening[:, :1] + dense_part * opening[:, LANES : LANES + 1]

    def swap(c):
        return remote(other.at[c], other_in.at[c], sws.at[c], swr.at[c], me, mate)

    for c in range(CHUNKS):

        @pl.loop(0, piece // step)
        def _(j, c=c):
            src = pl.ds(pl.multiple_of(mate * half + c * piece + j * step, step), step)
            other[c, :, pl.ds(pl.multiple_of(j * step, step), step)] = branch(src).astype(BF16)

        swap(c).start()

    def in_group(c, z, k, source):
        peer = lax.rem(i + k, INNER)
        return remote(
            summed.at[c, z, peer], plane_in.at[c, z, source], f1s.at[c, z, k], f1r.at[c, z, k],
            o * INNER + peer, tp,
        )

    def in_line(c, k, source):
        peer = lax.rem(o + k, outer)
        return remote(
            line_out.at[c, peer], line_in.at[c, source], f2s.at[c, k], f2r.at[c, k],
            peer * INNER + i, tp,
        )

    for c in range(CHUNKS):
        swap(c).wait()

        @pl.loop(0, piece // step)
        def _(j, c=c):
            src = pl.ds(pl.multiple_of(tp * half + c * piece + j * step, step), step)
            at = pl.ds(pl.multiple_of(j * step, step), step)
            both = branch(src) + other_in[c, :, at].astype(F32)
            summed[c, :, :, :, at] = both.astype(BF16).reshape(outer, INNER, seqs, step)

        @pl.loop(1, outer + 1)
        def _(k, c=c):
            z = lax.rem(o + k, outer)
            for j in range(1, INNER):
                in_group(c, z, j, i).start()

    for c in range(CHUNKS):

        @pl.loop(1, outer + 1)
        def _(k, c=c):
            z = lax.rem(o + k, outer)
            got = summed[c, z, i].astype(F32)
            for j in range(1, INNER):
                copy = in_group(c, z, j, lax.rem(i + INNER - j, INNER))
                copy.wait_send()
                copy.wait_recv()
                got = got + plane_in[c, z, lax.rem(i + INNER - j, INNER)].astype(F32)

            line_out[c, z] = got.astype(BF16)

            @pl.when(k < outer)
            def _():
                in_line(c, k, o).start()

    for c in range(CHUNKS):
        line_in[c, o] = line_out[c, o]

        @pl.loop(1, outer)
        def _(k, c=c):
            copy = in_line(c, k, lax.rem(o + outer - k, outer))
            copy.wait_send()
            copy.wait_recv()

        got = lax.fori_loop(
            0, outer, lambda z, carry, c=c: carry + line_in[c, z].astype(F32),
            jnp.zeros((seqs, piece), F32),
        )
        kept_row = row[:, pl.ds(pl.multiple_of(tp * half + c * piece, piece), piece)]
        final[:, c * piece : (c + 1) * piece] = (kept_row + got).astype(BF16)

    last = remote(final, final_in, fs, fr, me, mate)
    last.start()
    out_ref[:, pl.ds(pl.multiple_of(tp * half, half), half)] = final[...]
    last.wait()
    out_ref[:, pl.ds(pl.multiple_of(mate * half, half), half)] = final_in[...]


def layer(n, args):
    x, pos, freq, ids, weight, nmix, nffn, opened, gain, state = args[:10]
    wq, wout, eg, ed, dg, dd = args[10], args[14], args[15], args[17], args[18], args[20]
    seqs, width = x.shape
    heads, dim = state.shape[1], state.shape[2]
    hw, block, half, tokens = heads * dim, width // n, width // 2, n * seqs
    outer = n // INNER
    span, group, kb, piece = outer // 2, INNER * seqs, INNER * block, half // CHUNKS
    cols, dcols = eg.shape[2], dg.shape[1]
    vm, sem = pltpu.VMEM, pltpu.SemaphoreType.DMA
    vmem = pl.BlockSpec(memory_space=pltpu.VMEM)
    hbm = pl.BlockSpec(memory_space=pl.ANY)
    return pl.pallas_call(
        functools.partial(layer_kernel, n, heads, dim),
        out_shape=(
            jax.ShapeDtypeStruct((seqs, width), BF16),
            jax.ShapeDtypeStruct((seqs, hw), F32),
            jax.ShapeDtypeStruct((seqs, hw), BF16),
        ),
        in_specs=[hbm] * len(args),
        out_specs=(vmem, vmem, vmem),
        scratch_shapes=[
            vm(x.shape, BF16), pltpu.SMEM(pos.shape, jnp.int32), vm(freq.shape, F32),
            vm(ids.shape, jnp.int32), vm(weight.shape, BF16), vm(nmix.shape, BF16),
            vm(nffn.shape, BF16), vm(opened.shape, BF16), vm(gain.shape, BF16),
            vm(state.shape, F32), vm(eg.shape[1:], BF16), vm(eg.shape[1:], BF16),
            vm(ed.shape[1:], BF16), vm(dg.shape, BF16), vm(dg.shape, BF16), vm(dd.shape, BF16),
            vm((outer, seqs, kb), BF16),
            vm((n, seqs, kb), BF16),
            vm((INNER, block, hw), BF16),
            vm((2, span, hw, block), BF16),
            vm((2, hw, span * block), BF16),
            vm((outer, group, hw), BF16),
            vm((outer, group, hw), BF16),
            vm((INNER, seqs, hw), BF16),
            vm((INNER, seqs, hw), BF16),
            vm((1, hw), F32),
            vm((LANES, LANES), F32),
            vm((seqs, LANES), F32),
            vm((n, seqs, LANES), F32),
            vm((seqs, dim), F32), vm((seqs, dim), F32), vm((seqs, dim), F32),
            vm((seqs, hw), BF16),
            vm((2 * INNER, seqs, hw), BF16),
            vm((INNER, seqs, span * block), BF16),
            vm((2 * INNER, seqs, span * block), BF16),
            vm((seqs, width), F32),
            vm((2, seqs, half), BF16),
            vm((2, n, seqs, half), BF16),
            vm((LANES, width), BF16),
            vm((tokens, 2 * cols + 2 * dcols + LANES), F32),
            vm((tokens, cols), BF16),
            vm((tokens, dcols), BF16),
            vm((tokens, 2 * LANES), F32),
            vm((CHUNKS, tokens, piece), BF16),
            vm((CHUNKS, tokens, piece), BF16),
            vm((CHUNKS, outer, INNER, seqs, piece), BF16),
            vm((CHUNKS, outer, INNER, seqs, piece), BF16),
            vm((CHUNKS, outer, seqs, piece), BF16),
            vm((CHUNKS, outer, seqs, piece), BF16),
            vm((seqs, half), BF16),
            vm((seqs, half), BF16),
            sem((16,)),
            sem((n,)), sem((n,)),
            sem((INNER,)), sem((INNER,)), sem((2,)),
            sem((outer,)), sem((2, span)),
            sem((n,)), sem((n,)),
            sem((outer,)), sem((outer,)),
            sem((INNER,)), sem((INNER,)),
            sem((2 * INNER,)), sem((2 * INNER,)),
            sem((2 * INNER,)), sem((2 * INNER,)),
            sem((outer,)), sem((outer, INNER)), sem((n,)),
            sem((n,)), sem((n,)),
            sem((CHUNKS,)), sem((CHUNKS,)),
            sem((CHUNKS, outer, INNER)), sem((CHUNKS, outer, INNER)),
            sem((CHUNKS, outer)), sem((CHUNKS, outer)),
            sem, sem,
        ],
        compiler_params=pltpu.CompilerParams(
            collective_id=0, has_side_effects=True, vmem_limit_bytes=(40 if n <= 16 else 60) * 2**20
        ),
        name="layer",
    )(*args)


def update_kernel(heads, out_in, key_ref, value_ref, state_ref, out_ref, new_ref):
    h = pl.program_id(0)
    seqs = key_ref.shape[0]
    tp = lax.axis_index("tp")
    gamma = F32(0.0)
    for j in range(heads):
        low, high = decay(j, HEADS), decay(heads + j, HEADS)
        gamma = jnp.where(h == j, jnp.where(tp == 0, F32(low), F32(high)), gamma)

    @pl.when(h == 0)
    def _():
        out_ref[...] = out_in[...]

    key = key_ref[...].T
    value = value_ref[...].astype(F32)
    for s in range(seqs):
        new_ref[s, 0] = gamma * state_ref[s, 0] + key[:, s : s + 1] * value[s : s + 1, :]


def update(out, key, value, state):
    seqs, heads, dim = state.shape[:3]
    held = pl.BlockSpec((seqs, 1, dim, dim), lambda h: (0, h, 0, 0))
    piece = pl.BlockSpec((seqs, dim), lambda h: (0, h))
    whole = pl.BlockSpec(out.shape, lambda h: (0, 0))
    return pl.pallas_call(
        functools.partial(update_kernel, heads),
        grid=(heads,),
        out_shape=(
            jax.ShapeDtypeStruct(out.shape, BF16),
            jax.ShapeDtypeStruct(state.shape, F32),
        ),
        in_specs=[whole, piece, piece, held],
        out_specs=(whole, held),
        compiler_params=pltpu.CompilerParams(vmem_limit_bytes=16 * 2**20),
        name="update",
    )(out, key, value, state)


def on_device(
    inputs,
    positions,
    ret_state,
    norm_mix,
    w_query,
    w_key,
    w_value,
    w_gate_in,
    head_gain,
    w_out,
    norm_ffn,
    route_ids,
    route_weight,
    exp_gate,
    exp_up,
    exp_down,
    dense_gate,
    dense_up,
    dense_down,
    branch_gate,
):
    n = lax.axis_size("ep")
    dim = ret_state.shape[2]
    assert exp_gate.shape[0] == 1 and n % (2 * INNER) == 0 and n <= LANES
    turns = 10000.0 ** (-2.0 * np.arange(dim // 2) / dim)
    freq = jnp.asarray(np.concatenate([turns, turns])[None].astype(np.float32))
    out, key, value = layer(
        n,
        (inputs, positions, freq, route_ids.T, route_weight.T, norm_mix, norm_ffn, branch_gate,
         head_gain, ret_state, w_query, w_key, w_value, w_gate_in, w_out, exp_gate, exp_up,
         exp_down, dense_gate, dense_up, dense_down),
    )
    return update(out, key, value, ret_state)


def solution(mesh):
    in_specs = (
        P("ep", None),
        P("ep"),
        P("ep", "tp", None, None),
        P(),
        P("ep", "tp"),
        P("ep", "tp"),
        P("ep", "tp"),
        P("ep", "tp"),
        P("tp"),
        P("tp", "ep"),
        P(),
        P("ep", None),
        P("ep", None),
        P("ep", None, "tp"),
        P("ep", None, "tp"),
        P("ep", "tp", None),
        P(None, ("ep", "tp")),
        P(None, ("ep", "tp")),
        P(("ep", "tp"), None),
        P(),
    )
    out_specs = (P("ep", None), P("ep", "tp", None, None))
    return jax.shard_map(
        on_device, mesh=mesh, in_specs=in_specs, out_specs=out_specs, check_vma=False
    )
```

```python
import functools
import math

import jax
import jax.numpy as jnp
import numpy as np
from jax import lax
from jax.experimental import pallas as pl
from jax.experimental.pallas import tpu as pltpu
from jax.sharding import PartitionSpec as P

HEADS = 12
EPS = 1e-06
MESH = pl.DeviceIdType.MESH
LANES = 128
F32 = jnp.float32
BF16 = jnp.bfloat16
INNER = 4
CHUNKS = 2
WIDE = 256
PIECES = 3


def decay(head, head_count):
    return 1.0 - 2.0 ** (-5.0 - 5.0 * head / max(head_count - 1, 1))


def normalize(values, gain):
    return (values * lax.rsqrt(jnp.mean(values * values, axis=-1, keepdims=True) + EPS) * gain).astype(
        BF16
    )


def split(values):
    rest, pieces = values, []
    for _ in range(PIECES):
        pieces.append(rest.astype(BF16).astype(F32))
        rest = rest - pieces[-1]
    return jnp.concatenate(pieces, axis=0)


def remote(src, dst, send, recv, ep, tp):
    return pltpu.make_async_remote_copy(
        src_ref=src,
        dst_ref=dst,
        send_sem=send,
        recv_sem=recv,
        device_id=(ep, tp),
        device_id_type=MESH,
    )


def layer_kernel(
    n, heads, dim,
    x_hbm, pos_hbm, freq_hbm, ids_hbm, weight_hbm, nmix_hbm, nffn_hbm, open_hbm, gain_hbm,
    state_hbm, wq, wk, wv, wg, wout_hbm, eg_hbm, eu_hbm, ed_hbm, dg_hbm, du_hbm, dd_hbm,
    out_ref, key_ref, value_ref,
    x_ref, pos_ref, freq_ref, ids_ref, weight_ref, nmix_ref, nffn_ref, open_ref, gain_ref,
    state, eg, eu, ed, dg, du, dd,
    xsend, xrows, spread, wcol, wo, wo_flat, parts, zin, zsum, qkvg,
    gain_wide, table, share_rows, shares, cos_ref, sin_ref, readout, kept, heads_in,
    mixs, mixin, row, half_out, gathered, open_rows, acc, hidden, dense_hidden, opening,
    other, other_in, summed, plane_in, line_out, line_in, final, final_in,
    load, xs, xr, xm, ws, wr, local, outs, outr, shs, shr, zs, zr, ps, pr, cs, cr, ds, dr,
    ezs, eps, er, ms, mr, sws, swr, f1s, f1r, f2s, f2r, fs, fr,
):
    me, tp = lax.axis_index("ep"), lax.axis_index("tp")
    mate = 1 - tp
    outer = n // INNER
    span = INNER // 2
    o, i = me // INNER, lax.rem(me, INNER)
    seqs, width = x_ref.shape
    block, half, tokens, group = width // n, width // 2, n * seqs, INNER * seqs
    kb = INNER * block
    hw = heads * dim
    slabs, per_slab = hw // WIDE, WIDE // dim

    small = [
        pltpu.make_async_copy(src, dst, load.at[j])
        for j, (src, dst) in enumerate(
            ((x_hbm, x_ref), (nmix_hbm, nmix_ref), (ids_hbm, ids_ref), (weight_hbm, weight_ref),
             (pos_hbm, pos_ref), (freq_hbm, freq_ref), (nffn_hbm, nffn_ref), (open_hbm, open_ref),
             (gain_hbm, gain_ref))
        )
    ]
    large = [
        pltpu.make_async_copy(src, dst, load.at[len(small) + j])
        for j, (src, dst) in enumerate(
            ((state_hbm, state), (eg_hbm.at[0], eg), (eu_hbm.at[0], eu), (dg_hbm, dg),
             (du_hbm, du), (ed_hbm.at[0], ed), (dd_hbm, dd))
        )
    ]
    for copy in small:
        copy.start()

    barrier = pltpu.get_barrier_semaphore()

    def greet(ep, core):
        pl.semaphore_signal(barrier, inc=1, device_id=(ep, core), device_id_type=MESH)

    @pl.loop(1, n)
    def _(k):
        greet(lax.rem(me + k, n), tp)

    for j in range(INNER):
        greet(o * INNER + j, mate)

    @pl.loop(1, outer)
    def _(k):
        greet(lax.rem(o + k, outer) * INNER + i, mate)

    small[0].wait()
    small[1].wait()
    normed = normalize(x_ref[...].astype(F32), nmix_ref[...].astype(F32).reshape(1, width))
    for z in range(outer):
        for c in range(2):
            xsend[z, c] = normed[:, z * kb + c * (kb // 2) : z * kb + (c + 1) * (kb // 2)]
    pl.semaphore_wait(barrier, n - 1 + INNER + outer - 1)

    @pl.loop(1, n)
    def _(k):
        peer = lax.rem(me + k, n)
        remote(
            xsend.at[peer // INNER, tp], xrows.at[tp, me], xs.at[k], xr.at[k], peer, tp
        ).start()

    def rows_of(c, m, w, source):
        return remote(
            w.at[:, c * WIDE : (c + 1) * WIDE], wcol.at[c, source], ws.at[c, m], wr.at[c, source],
            o * INNER + m, tp,
        )

    def own_rows(c, m, w):
        return pltpu.make_async_copy(w.at[:, c * WIDE : (c + 1) * WIDE], wcol.at[c, m], local.at[c])

    for c in range(slabs):
        for m, w in enumerate((wq, wk, wv, wg)):

            @pl.when(i != m)
            def _(c=c, m=m, w=w):
                rows_of(c, m, w, i).start()

            @pl.when(i == m)
            def _(c=c, m=m, w=w):
                own_rows(c, m, w).start()

    holder, slot = i // span, lax.rem(i, span)

    def block_to(k):
        peer = lax.rem(i + k, INNER)
        return remote(
            wout_hbm, wo.at[tp, slot], outs.at[k], outr.at[tp, slot], o * INNER + peer, holder
        )

    own_wout = pltpu.make_async_copy(wout_hbm, wo.at[tp, slot], local.at[slabs])
    mate_wout = remote(wout_hbm, wo.at[tp, slot], outs.at[0], outr.at[tp, slot], me, mate)

    for k in range(1, INNER):
        block_to(k).start()

    @pl.when(holder == tp)
    def _():
        own_wout.start()

    @pl.when(holder != tp)
    def _():
        mate_wout.start()

    for copy in large:
        copy.start()
    xrows[tp, me] = xsend[o, tp]

    for j in (2, 3, 4, 5, 6, 7, 8):
        small[j].wait()
    widened = weight_ref[...].astype(F32)
    part = widened / jnp.sum(widened, axis=0, keepdims=True)
    expert = lax.broadcasted_iota(jnp.int32, (n, seqs), 0)
    named = jnp.zeros((n, seqs), F32)
    for j in range(ids_ref.shape[0]):
        named = named + jnp.where(ids_ref[j : j + 1, :] == expert, part[j : j + 1, :], 0.0)
    table[...] = jnp.zeros_like(table)
    table[:n, :seqs] = named
    for j in range(n):
        share_rows[j] = table[j : j + 1, :]

    def share_to(k, source):
        peer = lax.rem(me + k, n)
        return remote(share_rows.at[peer], shares.at[source], shs.at[k], shr.at[k], peer, tp)

    @pl.loop(1, n)
    def _(k):
        share_to(k, me).start()

    shares[me] = share_rows[me]

    rows_at = lax.broadcasted_iota(jnp.int32, (seqs, dim), 0)
    place = jnp.zeros((seqs, dim), F32)
    for s in range(seqs):
        place = jnp.where(rows_at == s, pos_ref[s].astype(F32), place)
    angles = place * freq_ref[...]
    lower = lax.broadcasted_iota(jnp.int32, (seqs, dim), 1) < dim // 2
    cos_ref[...] = jnp.cos(angles)
    sine = jnp.sin(angles)
    sin_ref[...] = jnp.where(lower, -sine, sine)
    open_rows[...] = jnp.broadcast_to(open_ref[...].astype(F32).reshape(1, width), open_rows.shape).astype(BF16)

    apart = lax.rem(lax.broadcasted_iota(jnp.int32, spread.shape, 0), seqs)
    spread[...] = jnp.where(
        apart == lax.broadcasted_iota(jnp.int32, spread.shape, 1) // dim, 1.0, 0.0
    ).astype(BF16)
    gain_wide[...] = gain_ref[...].astype(F32).reshape(1, hw)

    @pl.loop(1, n)
    def _(k):
        peer, came = lax.rem(me + k, n), lax.rem(me + n - k, n)
        copy = remote(
            xsend.at[peer // INNER, tp], xrows.at[tp, came], xs.at[k], xr.at[k], peer, tp
        )
        copy.wait_send()
        copy.wait_recv()

    def rows_to_mate(c):
        return remote(xrows.at[tp], xrows.at[c], xm.at[0], xm.at[1], me, mate)

    rows_to_mate(tp).start()

    def to_line(c, k, source):
        peer = lax.rem(o + k, outer)
        return remote(
            parts.at[c, peer], zin.at[c, source], zs.at[c, k], zr.at[c, k], peer * INNER + i, tp
        )

    for c in range(slabs):
        for m, w in enumerate((wq, wk, wv, wg)):

            @pl.when(i != m)
            def _(c=c, m=m, w=w):
                copy = rows_of(c, m, w, m)
                copy.wait_send()
                copy.wait_recv()

            @pl.when(i == m)
            def _(c=c, m=m, w=w):
                own_rows(c, m, w).wait()

        if c == 0:
            swapped = rows_to_mate(mate)
            swapped.wait_send()
            swapped.wait_recv()
        product = sum(
            jnp.dot(
                xrows[q].reshape(tokens, kb // 2),
                wcol[c, q * 2 : q * 2 + 2].reshape(kb // 2, WIDE),
                preferred_element_type=F32,
            )
            for q in range(2)
        )
        parts[c] = product.astype(BF16).reshape(outer, group, WIDE)

        @pl.loop(1, outer)
        def _(k, c=c):
            to_line(c, k, o).start()

    def to_plane(c, k, source):
        peer = lax.rem(i + k, INNER)
        return remote(
            zsum.at[c, peer], qkvg.at[c, source], ps.at[c, k], pr.at[c, k], o * INNER + peer, tp
        )

    def head(c, q):
        h = c * per_slab + q
        at = slice(q * dim, (q + 1) * dim)
        gamma = jnp.where(tp == 0, F32(decay(h, HEADS)), F32(decay(heads + h, HEADS)))

        def rotated(j):
            val = qkvg[c, j, :, at].astype(F32)
            return val * cos_ref[...] + pltpu.roll(val, dim // 2, 1) * sin_ref[...]

        query = rotated(0)
        key = rotated(1) * dim ** (-0.5)
        key_ref[:, h * dim : (h + 1) * dim] = key
        value = qkvg[c, 2, :, at].astype(F32)
        value_ref[:, h * dim : (h + 1) * dim] = qkvg[c, 2, :, at]
        across = split(query).T.astype(BF16)
        for s in range(0, seqs, 2):
            wide = jnp.dot(
                across, spread[:, s * dim : (s + 2) * dim], preferred_element_type=F32
            )
            for t in range(2):
                readout[s + t : s + t + 1, :] = jnp.sum(
                    state[s + t, h] * wide[:, t * dim : (t + 1) * dim], axis=0, keepdims=True
                )
        read = gamma * readout[...] + jnp.sum(query * key, axis=-1, keepdims=True) * value
        centred = read - jnp.mean(read, axis=-1, keepdims=True)
        scaled = centred * lax.rsqrt(jnp.mean(centred * centred, axis=-1, keepdims=True) + EPS)
        gate = qkvg[c, 3, :, at].astype(F32)
        gain = gain_wide[:, h * dim : (h + 1) * dim]
        kept[c, :, at] = (scaled * gain * (gate * jax.nn.sigmoid(gate))).astype(BF16)

    mine = tp * outer + o

    def to_cores(src, dst, send, recv, j):
        core = lax.rem(tp + j // outer, 2)
        peer = lax.rem(o + lax.rem(j, outer), outer)
        return remote(src(peer), dst, send.at[j], recv.at[j], peer * INNER + i, core)

    def source_of(j):
        core = lax.rem(tp + 2 - j // outer, 2)
        return core * outer + lax.rem(o + outer - lax.rem(j, outer), outer)

    def kept_to(c, j, source):
        return to_cores(lambda p: kept.at[c], heads_in.at[c, source], cs.at[c], cr.at[c], j)

    def retain(c):
        for k in range(1, INNER):
            copy = to_plane(c, k, lax.rem(i + INNER - k, INNER))
            copy.wait_send()
            copy.wait_recv()
        for q in range(per_slab):
            head(c, q)

        @pl.loop(1, 2 * outer)
        def _(j):
            kept_to(c, j, mine).start()

        heads_in[c, mine] = kept[c]

    large[0].wait()
    for c in range(slabs):

        @pl.loop(1, outer)
        def _(k, c=c):
            copy = to_line(c, k, lax.rem(o + outer - k, outer))
            copy.wait_send()
            copy.wait_recv()

        zin[c, o] = parts[c, o]
        total = lax.fori_loop(
            0, outer, lambda z, carry, c=c: carry + zin[c, z].astype(F32),
            jnp.zeros((group, WIDE), F32),
        )
        zsum[c] = total.astype(BF16).reshape(INNER, seqs, WIDE)
        for k in range(1, INNER):
            to_plane(c, k, i).start()
        qkvg[c, i] = zsum[c, i]
        if c > 0:
            retain(c - 1)
    retain(slabs - 1)

    for k in range(1, INNER):
        block_to(k).wait_send()

    @pl.when(holder == tp)
    def _():
        own_wout.wait()

    @pl.when(holder != tp)
    def _():
        mate_wout.wait_send()

    for core in range(2):
        for s in range(span):

            @pl.when(jnp.logical_not(jnp.logical_and(core == tp, tp * span + s == i)))
            def _(core=core, s=s):
                remote(
                    wout_hbm, wo.at[core, s], outs.at[0], outr.at[core, s], me, mate
                ).wait_recv()

            wo_flat[core, :, s * block : (s + 1) * block] = wo[core, s]

    for c in range(slabs):

        @pl.loop(1, 2 * outer)
        def _(j, c=c):
            copy = kept_to(c, j, source_of(j))
            copy.wait_send()
            copy.wait_recv()

    first, second = (
        sum(
            jnp.dot(
                heads_in[c, q * outer : (q + 1) * outer].reshape(outer * seqs, WIDE),
                wo_flat[q, c * WIDE : (c + 1) * WIDE, :],
                preferred_element_type=F32,
            )
            for c in range(slabs)
        ).astype(BF16)
        for q in range(2)
    )
    mixs[...] = (first.astype(F32) + second.astype(F32)).astype(BF16).reshape(
        outer, seqs, span * block
    )

    def mixed_to(j, source):
        return to_cores(lambda p: mixs.at[p], mixin.at[source], ds, dr, j)

    @pl.loop(1, 2 * outer)
    def _(j):
        mixed_to(j, mine).start()

    mixin[mine] = mixs[o]
    @pl.loop(1, 2 * outer)
    def _(j):
        copy = mixed_to(j, source_of(j))
        copy.wait_send()
        copy.wait_recv()

    for z in range(outer):
        for j in range(INNER):
            b = z * INNER + j
            row[:, b * block : (b + 1) * block] = mixin[
                (j // span) * outer + z, :, (j % span) * block : (j % span + 1) * block
            ].astype(F32)
    residual = (x_ref[...].astype(F32) + row[...]).astype(BF16).astype(F32)
    row[...] = residual
    normed = normalize(residual, nffn_ref[...].astype(F32).reshape(1, width))
    for c in range(2):
        half_out[c] = normed[:, c * half : (c + 1) * half]

    def along(peer, block_id):
        return remote(
            half_out.at[tp], gathered.at[tp, block_id], ezs.at[peer], er.at[block_id],
            peer * INNER + i, tp,
        )

    def inside(src, k, z, block_id):
        peer = lax.rem(i + k, INNER)
        return remote(
            src, gathered.at[tp, block_id], eps.at[z, k], er.at[block_id], o * INNER + peer, tp
        )

    def across_cores(half_id, block_id):
        return remote(
            gathered.at[tp, block_id], gathered.at[half_id, block_id], ms.at[block_id],
            mr.at[block_id], me, mate,
        )

    def on_line(far, act):
        for sign in (1, -1):
            peer = o + sign * far

            @pl.when(jnp.logical_and(peer >= 0, peer < outer))
            def _(peer=peer):
                act(peer)

    @pl.loop(1, outer)
    def _(d):
        on_line(outer - d, lambda peer: along(peer, me).start())

    for k in range(1, INNER):
        inside(half_out.at[tp], k, o, me).start()
    for c in range(2):
        gathered[c, me] = half_out[c]

    def from_group(z):
        for j in range(1, INNER):
            came = z * INNER + lax.rem(i + INNER - j, INNER)
            inside(half_out.at[tp], j, z, came).wait_recv()
            across_cores(tp, came).start()

    def relay(peer):
        came = peer * INNER + i
        along(peer, came).wait_recv()
        for j in range(1, INNER):
            inside(gathered.at[tp, came], j, peer, came).start()
        across_cores(tp, came).start()

    cols = eg.shape[1]
    dcols = dg.shape[1]
    tile = min(256, cols)
    wide = 2 * cols
    part_rows = tokens // 2
    near = o // (outer // 2)

    def half_dot(g, c, first):
        per = n // 2
        left = gathered[c, pl.ds(g * per, per)].reshape(part_rows, half)
        k_at = pl.ds(pl.multiple_of(c * half, half), half)
        rows = pl.ds(pl.multiple_of(g * part_rows, part_rows), part_rows)

        def put(at, value):
            if first:
                acc[rows, at] = value
            else:
                acc[rows, at] += value

        for base, w in ((0, eg), (cols, eu)):

            @pl.loop(0, cols // tile)
            def _(j, base=base, w=w):
                src = pl.ds(pl.multiple_of(j * tile, tile), tile)
                dst = pl.ds(pl.multiple_of(base + j * tile, tile), tile)
                put(dst, jnp.dot(left, w[k_at, src], preferred_element_type=F32))

        for base, w in ((wide, dg), (wide + dcols, du)):
            put(slice(base, base + dcols), jnp.dot(left, w[k_at, :], preferred_element_type=F32))
        put(
            slice(wide + 2 * dcols, wide + 2 * dcols + LANES),
            lax.dot_general(
                left, open_rows[:, k_at], (((1,), (1,)), ((), ())), preferred_element_type=F32
            ),
        )

    def from_mate(g):
        @pl.loop(0, n // 2)
        def _(q):
            block_id = g * (n // 2) + q

            @pl.when(block_id != me)
            def _():
                copy = across_cores(mate, block_id)
                copy.wait_send()
                copy.wait_recv()

    @pl.loop(1, outer)
    def _(d):
        on_line(d, relay)

    @pl.loop(0, outer // 2)
    def _(z):
        from_group(near * (outer // 2) + z)

    for copy in large[1:]:
        copy.wait()

    half_dot(near, tp, True)
    from_mate(near)
    half_dot(near, mate, False)
    away = 1 - near

    @pl.loop(0, outer // 2)
    def _(z):
        from_group(away * (outer // 2) + z)

    half_dot(away, tp, True)
    from_mate(away)
    half_dot(away, mate, False)

    @pl.loop(1, outer)
    def _(d):
        on_line(d, lambda peer: along(peer, me).wait_send())

    @pl.loop(0, outer)
    def _(z):
        for j in range(1, INNER):
            inside(half_out.at[tp], j, z, me).wait_send()

    @pl.loop(1, n)
    def _(k):
        copy = share_to(k, lax.rem(me + n - k, n))
        copy.wait_send()
        copy.wait_recv()

    for j in range(n):
        table[j : j + 1, :] = shares[j]
    columns = table[...].T[:seqs]
    for j in range(n):
        opening[j * seqs : (j + 1) * seqs, :LANES] = jnp.broadcast_to(
            columns[:, j : j + 1], (seqs, LANES)
        )
    opening[:, LANES:] = jax.nn.sigmoid(acc[:, wide + 2 * dcols : wide + 2 * dcols + LANES])

    @pl.loop(0, cols // tile)
    def _(j):
        at = pl.ds(pl.multiple_of(j * tile, tile), tile)
        gate, up = acc[:, at], acc[:, pl.ds(pl.multiple_of(cols + j * tile, tile), tile)]
        hidden[:, at] = (gate * jax.nn.sigmoid(gate) * up).astype(BF16)

    gate = acc[:, wide : wide + dcols]
    dense_hidden[...] = (
        gate * jax.nn.sigmoid(gate) * acc[:, wide + dcols : wide + 2 * dcols]
    ).astype(BF16)

    piece = half // CHUNKS
    step = min(256, piece)

    def branch(at):
        expert_part = jnp.dot(hidden[...], ed[:, at], preferred_element_type=F32)
        dense_part = jnp.dot(dense_hidden[...], dd[:, at], preferred_element_type=F32)
        return expert_part * opening[:, :1] + dense_part * opening[:, LANES : LANES + 1]

    def swap(c):
        return remote(other.at[c], other_in.at[c], sws.at[c], swr.at[c], me, mate)

    for c in range(CHUNKS):

        @pl.loop(0, piece // step)
        def _(j, c=c):
            src = pl.ds(pl.multiple_of(mate * half + c * piece + j * step, step), step)
            other[c, :, pl.ds(pl.multiple_of(j * step, step), step)] = branch(src).astype(BF16)

        swap(c).start()

    def in_group(c, z, k, source):
        peer = lax.rem(i + k, INNER)
        return remote(
            summed.at[c, z, peer], plane_in.at[c, z, source], f1s.at[c, z, k], f1r.at[c, z, k],
            o * INNER + peer, tp,
        )

    def in_line(c, k, source):
        peer = lax.rem(o + k, outer)
        return remote(
            line_out.at[c, peer], line_in.at[c, source], f2s.at[c, k], f2r.at[c, k],
            peer * INNER + i, tp,
        )

    for c in range(CHUNKS):
        swap(c).wait()

        @pl.loop(0, piece // step)
        def _(j, c=c):
            src = pl.ds(pl.multiple_of(tp * half + c * piece + j * step, step), step)
            at = pl.ds(pl.multiple_of(j * step, step), step)
            both = branch(src) + other_in[c, :, at].astype(F32)
            summed[c, :, :, :, at] = both.astype(BF16).reshape(outer, INNER, seqs, step)

        @pl.loop(1, outer + 1)
        def _(k, c=c):
            z = lax.rem(o + k, outer)
            for j in range(1, INNER):
                in_group(c, z, j, i).start()

    for c in range(CHUNKS):

        @pl.loop(1, outer + 1)
        def _(k, c=c):
            z = lax.rem(o + k, outer)
            got = summed[c, z, i].astype(F32)
            for j in range(1, INNER):
                copy = in_group(c, z, j, lax.rem(i + INNER - j, INNER))
                copy.wait_send()
                copy.wait_recv()
                got = got + plane_in[c, z, lax.rem(i + INNER - j, INNER)].astype(F32)

            line_out[c, z] = got.astype(BF16)

            @pl.when(k < outer)
            def _():
                in_line(c, k, o).start()

    for c in range(CHUNKS):
        line_in[c, o] = line_out[c, o]

        @pl.loop(1, outer)
        def _(k, c=c):
            copy = in_line(c, k, lax.rem(o + outer - k, outer))
            copy.wait_send()
            copy.wait_recv()

        got = lax.fori_loop(
            0, outer, lambda z, carry, c=c: carry + line_in[c, z].astype(F32),
            jnp.zeros((seqs, piece), F32),
        )
        kept_row = row[:, pl.ds(pl.multiple_of(tp * half + c * piece, piece), piece)]
        final[:, c * piece : (c + 1) * piece] = (kept_row + got).astype(BF16)

    last = remote(final, final_in, fs, fr, me, mate)
    last.start()
    out_ref[:, pl.ds(pl.multiple_of(tp * half, half), half)] = final[...]
    last.wait()
    out_ref[:, pl.ds(pl.multiple_of(mate * half, half), half)] = final_in[...]


def layer(n, args):
    x, pos, freq, ids, weight, nmix, nffn, opened, gain, state = args[:10]
    wq, wout, eg, ed, dg, dd = args[10], args[14], args[15], args[17], args[18], args[20]
    seqs, width = x.shape
    heads, dim = state.shape[1], state.shape[2]
    hw, block, half, tokens = heads * dim, width // n, width // 2, n * seqs
    outer = n // INNER
    span, group, kb, piece = INNER // 2, INNER * seqs, INNER * block, half // CHUNKS
    slabs = hw // WIDE
    cols, dcols = eg.shape[2], dg.shape[1]
    vm, sem = pltpu.VMEM, pltpu.SemaphoreType.DMA
    vmem = pl.BlockSpec(memory_space=pltpu.VMEM)
    hbm = pl.BlockSpec(memory_space=pltpu.HBM)
    return pl.pallas_call(
        functools.partial(layer_kernel, n, heads, dim),
        out_shape=(
            jax.ShapeDtypeStruct((seqs, width), BF16),
            jax.ShapeDtypeStruct((seqs, hw), F32),
            jax.ShapeDtypeStruct((seqs, hw), BF16),
        ),
        in_specs=[hbm] * len(args),
        out_specs=(vmem, vmem, vmem),
        scratch_shapes=[
            vm(x.shape, BF16), pltpu.SMEM(pos.shape, jnp.int32), vm(freq.shape, F32),
            vm(ids.shape, jnp.int32), vm(weight.shape, BF16), vm(nmix.shape, BF16),
            vm(nffn.shape, BF16), vm(opened.shape, BF16), vm(gain.shape, BF16),
            vm(state.shape, F32), vm(eg.shape[1:], BF16), vm(eg.shape[1:], BF16),
            vm(ed.shape[1:], BF16), vm(dg.shape, BF16), vm(dg.shape, BF16), vm(dd.shape, BF16),
            vm((outer, 2, seqs, kb // 2), BF16),
            vm((2, n, seqs, kb // 2), BF16),
            vm((PIECES * seqs, seqs * dim), BF16),
            vm((slabs, INNER, block, WIDE), BF16),
            vm((2, span, hw, block), BF16),
            vm((2, hw, span * block), BF16),
            vm((slabs, outer, group, WIDE), BF16),
            vm((slabs, outer, group, WIDE), BF16),
            vm((slabs, INNER, seqs, WIDE), BF16),
            vm((slabs, INNER, seqs, WIDE), BF16),
            vm((1, hw), F32),
            vm((LANES, LANES), F32),
            vm((n, 1, LANES), F32),
            vm((n, 1, LANES), F32),
            vm((seqs, dim), F32), vm((seqs, dim), F32), vm((seqs, dim), F32),
            vm((slabs, seqs, WIDE), BF16),
            vm((slabs, 2 * outer, seqs, WIDE), BF16),
            vm((outer, seqs, span * block), BF16),
            vm((2 * outer, seqs, span * block), BF16),
            vm((seqs, width), F32),
            vm((2, seqs, half), BF16),
            vm((2, n, seqs, half), BF16),
            vm((LANES, width), BF16),
            vm((tokens, 2 * cols + 2 * dcols + LANES), F32),
            vm((tokens, cols), BF16),
            vm((tokens, dcols), BF16),
            vm((tokens, 2 * LANES), F32),
            vm((CHUNKS, tokens, piece), BF16),
            vm((CHUNKS, tokens, piece), BF16),
            vm((CHUNKS, outer, INNER, seqs, piece), BF16),
            vm((CHUNKS, outer, INNER, seqs, piece), BF16),
            vm((CHUNKS, outer, seqs, piece), BF16),
            vm((CHUNKS, outer, seqs, piece), BF16),
            vm((seqs, half), BF16),
            vm((seqs, half), BF16),
            sem((16,)),
            sem((n,)), sem((n,)), sem((2,)),
            sem((slabs, INNER)), sem((slabs, INNER)), sem((slabs + 1,)),
            sem((INNER,)), sem((2, span)),
            sem((n,)), sem((n,)),
            sem((slabs, outer)), sem((slabs, outer)),
            sem((slabs, INNER)), sem((slabs, INNER)),
            sem((slabs, 2 * outer)), sem((slabs, 2 * outer)),
            sem((2 * outer,)), sem((2 * outer,)),
            sem((outer,)), sem((outer, INNER)), sem((n,)),
            sem((n,)), sem((n,)),
            sem((CHUNKS,)), sem((CHUNKS,)),
            sem((CHUNKS, outer, INNER)), sem((CHUNKS, outer, INNER)),
            sem((CHUNKS, outer)), sem((CHUNKS, outer)),
            sem, sem,
        ],
        compiler_params=pltpu.CompilerParams(
            collective_id=0, has_side_effects=True, vmem_limit_bytes=60 * 2**20
        ),
        name="layer",
    )(*args)


def update_kernel(heads, out_in, key_ref, value_ref, state_ref, out_ref, new_ref):
    seqs = key_ref.shape[0]
    dim = value_ref.shape[1] // heads
    tp = lax.axis_index("tp")

    @pl.when(pl.program_id(0) == 0)
    def _():
        out_ref[...] = out_in[...]

    row = lax.broadcasted_iota(jnp.int32, (seqs, 2 * dim), 0)
    lane = lax.broadcasted_iota(jnp.int32, (seqs, 2 * dim), 1) // dim
    for h in range(heads):
        gamma = jnp.where(tp == 0, F32(decay(h, HEADS)), F32(decay(heads + h, HEADS)))
        at = slice(h * dim, (h + 1) * dim)
        key = split(key_ref[:, at]).T.astype(BF16)
        value = value_ref[:, at].astype(F32)
        twice = jnp.concatenate([value, value], axis=1)
        for s in range(0, seqs, 2):
            spread = jnp.where(row == s + lane, twice, 0.0)
            spread = jnp.concatenate([spread] * PIECES, axis=0).astype(BF16)
            added = jnp.dot(key, spread, preferred_element_type=F32)
            for t in range(2):
                new_ref[s + t, h] = gamma * state_ref[s + t, h] + added[:, t * dim : (t + 1) * dim]


def update(out, key, value, state):
    seqs, heads, dim = state.shape[:3]
    few = min(8, seqs)
    held = pl.BlockSpec((few, heads, dim, dim), lambda j: (j, 0, 0, 0))
    piece = pl.BlockSpec((few, heads * dim), lambda j: (j, 0))
    whole = pl.BlockSpec(out.shape, lambda j: (0, 0))
    return pl.pallas_call(
        functools.partial(update_kernel, heads),
        grid=(seqs // few,),
        out_shape=(
            jax.ShapeDtypeStruct(out.shape, BF16),
            jax.ShapeDtypeStruct(state.shape, F32),
        ),
        in_specs=[whole, piece, piece, held],
        out_specs=(whole, held),
        compiler_params=pltpu.CompilerParams(vmem_limit_bytes=60 * 2**20),
        name="update",
    )(out, key, value, state)


def on_device(
    inputs,
    positions,
    ret_state,
    norm_mix,
    w_query,
    w_key,
    w_value,
    w_gate_in,
    head_gain,
    w_out,
    norm_ffn,
    route_ids,
    route_weight,
    exp_gate,
    exp_up,
    exp_down,
    dense_gate,
    dense_up,
    dense_down,
    branch_gate,
):
    n = lax.axis_size("ep")
    dim = ret_state.shape[2]
    assert exp_gate.shape[0] == 1 and n % (2 * INNER) == 0 and n <= LANES
    assert w_query.shape[1] % WIDE == 0 and WIDE % dim == 0
    turns = 10000.0 ** (-2.0 * np.arange(dim // 2) / dim)
    freq = jnp.asarray(np.concatenate([turns, turns])[None].astype(np.float32))
    out, key, value = layer(
        n,
        (inputs, positions, freq, route_ids.T, route_weight.T, norm_mix, norm_ffn, branch_gate,
         head_gain, ret_state, w_query, w_key, w_value, w_gate_in, w_out, exp_gate, exp_up,
         exp_down, dense_gate, dense_up, dense_down),
    )
    return update(out, key, value, ret_state)


def solution(mesh):
    in_specs = (
        P("ep", None),
        P("ep"),
        P("ep", "tp", None, None),
        P(),
        P("ep", "tp"),
        P("ep", "tp"),
        P("ep", "tp"),
        P("ep", "tp"),
        P("tp"),
        P("tp", "ep"),
        P(),
        P("ep", None),
        P("ep", None),
        P("ep", None, "tp"),
        P("ep", None, "tp"),
        P("ep", "tp", None),
        P(None, ("ep", "tp")),
        P(None, ("ep", "tp")),
        P(("ep", "tp"), None),
        P(),
    )
    out_specs = (P("ep", None), P("ep", "tp", None, None))
    return jax.shard_map(
        on_device, mesh=mesh, in_specs=in_specs, out_specs=out_specs, check_vma=False
    )
```

```python
import functools
import math

import jax
import jax.numpy as jnp
import numpy as np
from jax import lax
from jax.experimental import pallas as pl
from jax.experimental.pallas import tpu as pltpu
from jax.sharding import PartitionSpec as P

HEADS = 12
EPS = 1e-06
MESH = pl.DeviceIdType.MESH
LANES = 128
F32 = jnp.float32
BF16 = jnp.bfloat16
INNER = 4
CHUNKS = 2
WIDE = 384
PIECES = 3


def decay(head, head_count):
    return 1.0 - 2.0 ** (-5.0 - 5.0 * head / max(head_count - 1, 1))


def normalize(values, gain):
    return (values * lax.rsqrt(jnp.mean(values * values, axis=-1, keepdims=True) + EPS) * gain).astype(
        BF16
    )


def split(values):
    rest, pieces = values, []
    for _ in range(PIECES):
        pieces.append(rest.astype(BF16).astype(F32))
        rest = rest - pieces[-1]
    return jnp.concatenate(pieces, axis=0)


def remote(src, dst, send, recv, ep, tp):
    return pltpu.make_async_remote_copy(
        src_ref=src,
        dst_ref=dst,
        send_sem=send,
        recv_sem=recv,
        device_id=(ep, tp),
        device_id_type=MESH,
    )


def layer_kernel(
    n, heads, dim,
    x_hbm, pos_hbm, freq_hbm, ids_hbm, weight_hbm, nmix_hbm, nffn_hbm, open_hbm, gain_hbm,
    state_hbm, wq, wk, wv, wg, wout_hbm, eg_hbm, eu_hbm, ed_hbm, dg_hbm, du_hbm, dd_hbm,
    out_ref, key_ref, value_ref,
    x_ref, pos_ref, freq_ref, ids_ref, weight_ref, nmix_ref, nffn_ref, open_ref, gain_ref,
    state, eg, eu, ed, dg, du, dd,
    xsend, xrows, spread, wcol, wo, wo_flat, parts, zin, qkvg,
    gain_wide, table, share_rows, shares, cos_ref, sin_ref, readout, kept, heads_in,
    raw, xline, rblock, row, gathered, nffn_wide, open_rows, squares, scales, acc, hidden, dense_hidden, opening,
    other, other_in, own, summed, plane_in, line_out, line_in, final, final_in,
    load, xs, xr, xm, ws, wr, local, outs, outr, shs, shr, zs, zr, cs, cr, xls, xlr,
    ezs, eps, er, ms, mr, sws, swr, f1s, f1r, f2s, f2r, fs, fr,
):
    me, tp = lax.axis_index("ep"), lax.axis_index("tp")
    mate = 1 - tp
    outer = n // INNER
    span = INNER // 2
    o, i = me // INNER, lax.rem(me, INNER)
    seqs, width = x_ref.shape
    block, half, tokens, group = width // n, width // 2, n * seqs, INNER * seqs
    kb = INNER * block
    hw = heads * dim
    slabs, per_slab = hw // WIDE, WIDE // dim

    small = [
        pltpu.make_async_copy(src, dst, load.at[j])
        for j, (src, dst) in enumerate(
            ((x_hbm, x_ref), (nmix_hbm, nmix_ref), (ids_hbm, ids_ref), (weight_hbm, weight_ref),
             (pos_hbm, pos_ref), (freq_hbm, freq_ref), (nffn_hbm, nffn_ref), (open_hbm, open_ref),
             (gain_hbm, gain_ref))
        )
    ]
    large = [
        pltpu.make_async_copy(src, dst, load.at[len(small) + j])
        for j, (src, dst) in enumerate(
            ((state_hbm, state), (eg_hbm.at[0], eg), (eu_hbm.at[0], eu), (dg_hbm, dg),
             (du_hbm, du), (ed_hbm.at[0], ed), (dd_hbm, dd))
        )
    ]
    for copy in small:
        copy.start()

    def on_line(far, act):
        for sign in (1, -1):
            peer = o + sign * far

            @pl.when(jnp.logical_and(peer >= 0, peer < outer))
            def _(peer=peer):
                act(peer)

    barrier = pltpu.get_barrier_semaphore()

    def greet(ep, core):
        pl.semaphore_signal(barrier, inc=1, device_id=(ep, core), device_id_type=MESH)

    @pl.loop(1, n)
    def _(k):
        greet(lax.rem(me + k, n), tp)

    for j in range(INNER):
        greet(o * INNER + j, mate)

    @pl.loop(1, outer)
    def _(k):
        greet(lax.rem(o + k, outer) * INNER + i, mate)

    small[0].wait()
    small[1].wait()
    normed = normalize(x_ref[...].astype(F32), nmix_ref[...].astype(F32).reshape(1, width))
    for z in range(outer):
        for c in range(2):
            at = slice(z * kb + c * (kb // 2), z * kb + (c + 1) * (kb // 2))
            xsend[z, c] = normed[:, at]
            raw[z, c] = x_ref[:, at]
    pl.semaphore_wait(barrier, n - 1 + INNER + outer - 1)

    @pl.loop(1, n)
    def _(k):
        peer = lax.rem(me + k, n)
        remote(
            xsend.at[peer // INNER, tp], xrows.at[tp, me], xs.at[k], xr.at[k], peer, tp
        ).start()

    def rows_of(c, m, w, source):
        return remote(
            w.at[:, c * WIDE : (c + 1) * WIDE], wcol.at[c, source], ws.at[c, m], wr.at[c, source],
            o * INNER + m, tp,
        )

    def own_rows(c, m, w):
        return pltpu.make_async_copy(w.at[:, c * WIDE : (c + 1) * WIDE], wcol.at[c, m], local.at[c])

    for c in range(slabs):
        for m, w in enumerate((wq, wk, wv, wg)):

            @pl.when(i != m)
            def _(c=c, m=m, w=w):
                rows_of(c, m, w, i).start()

            @pl.when(i == m)
            def _(c=c, m=m, w=w):
                own_rows(c, m, w).start()

    holder, slot = i // span, lax.rem(i, span)

    def block_to(k):
        peer = lax.rem(i + k, INNER)
        return remote(
            wout_hbm, wo.at[tp, slot], outs.at[k], outr.at[tp, slot], o * INNER + peer, holder
        )

    own_wout = pltpu.make_async_copy(wout_hbm, wo.at[tp, slot], local.at[slabs])
    mate_wout = remote(wout_hbm, wo.at[tp, slot], outs.at[0], outr.at[tp, slot], me, mate)

    def columns_to(k, source):
        peer = lax.rem(o + k, outer)
        return remote(
            raw.at[peer, tp], xline.at[source], xls.at[k], xlr.at[k], peer * INNER + i, tp
        )

    @pl.loop(1, outer)
    def _(k):
        columns_to(k, o).start()

    xline[o] = raw[o, tp]
    for copy in large:
        copy.start()
    xrows[tp, me] = xsend[o, tp]

    for j in (2, 3, 4, 5, 6, 7, 8):
        small[j].wait()
    widened = weight_ref[...].astype(F32)
    part = widened / jnp.sum(widened, axis=0, keepdims=True)
    expert = lax.broadcasted_iota(jnp.int32, (n, seqs), 0)
    named = jnp.zeros((n, seqs), F32)
    for j in range(ids_ref.shape[0]):
        named = named + jnp.where(ids_ref[j : j + 1, :] == expert, part[j : j + 1, :], 0.0)
    table[...] = jnp.zeros_like(table)
    table[:n, :seqs] = named
    for j in range(n):
        share_rows[j] = table[j : j + 1, :]

    def share_to(k, source):
        peer = lax.rem(me + k, n)
        return remote(share_rows.at[peer], shares.at[source], shs.at[k], shr.at[k], peer, tp)

    @pl.loop(1, n)
    def _(k):
        share_to(k, me).start()

    shares[me] = share_rows[me]

    rows_at = lax.broadcasted_iota(jnp.int32, (seqs, dim), 0)
    place = jnp.zeros((seqs, dim), F32)
    for s in range(seqs):
        place = jnp.where(rows_at == s, pos_ref[s].astype(F32), place)
    angles = place * freq_ref[...]
    lower = lax.broadcasted_iota(jnp.int32, (seqs, dim), 1) < dim // 2
    cos_ref[...] = jnp.cos(angles)
    sine = jnp.sin(angles)
    sin_ref[...] = jnp.where(lower, -sine, sine)
    gains = nffn_ref[...].astype(F32).reshape(1, width)
    opens = open_ref[...].astype(F32).reshape(1, width)
    for z in range(outer):
        for c in range(2):
            at = slice(z * kb + c * (kb // 2), z * kb + (c + 1) * (kb // 2))
            nffn_wide[z, c] = gains[:, at]
            open_rows[z, c] = jnp.broadcast_to(opens[:, at], (LANES, kb // 2)).astype(BF16)
    apart = lax.rem(lax.broadcasted_iota(jnp.int32, spread.shape, 0), seqs)
    spread[...] = jnp.where(
        apart == lax.broadcasted_iota(jnp.int32, spread.shape, 1) // dim, 1.0, 0.0
    ).astype(BF16)
    gain_wide[...] = gain_ref[...].astype(F32).reshape(1, hw)

    @pl.loop(1, n)
    def _(k):
        peer, came = lax.rem(me + k, n), lax.rem(me + n - k, n)
        copy = remote(
            xsend.at[peer // INNER, tp], xrows.at[tp, came], xs.at[k], xr.at[k], peer, tp
        )
        copy.wait_send()
        copy.wait_recv()

    def rows_to_mate(c):
        return remote(xrows.at[tp], xrows.at[c], xm.at[0], xm.at[1], me, mate)

    rows_to_mate(tp).start()

    def to_owner(c, peer, source):
        return remote(
            parts.at[c, peer], zin.at[c, source], zs.at[c, peer], zr.at[c, source], peer, tp
        )

    def scatter(c):
        @pl.loop(1, outer)
        def _(d):
            def send(z):
                for j in range(INNER):
                    to_owner(c, z * INNER + j, me).start()

            on_line(outer - d, send)

        for k in range(1, INNER):
            to_owner(c, o * INNER + lax.rem(i + k, INNER), me).start()

    for c in range(slabs):
        for m, w in enumerate((wq, wk, wv, wg)):

            @pl.when(i != m)
            def _(c=c, m=m, w=w):
                copy = rows_of(c, m, w, m)
                copy.wait_send()
                copy.wait_recv()

            @pl.when(i == m)
            def _(c=c, m=m, w=w):
                own_rows(c, m, w).wait()

        if c == 0:
            swapped = rows_to_mate(mate)
            swapped.wait_send()
            swapped.wait_recv()
        product = sum(
            jnp.dot(
                xrows[q].reshape(tokens, kb // 2),
                wcol[c, q * 2 : q * 2 + 2].reshape(kb // 2, WIDE),
                preferred_element_type=F32,
            )
            for q in range(2)
        )
        parts[c] = product.astype(BF16).reshape(n, seqs, WIDE)
        scatter(c)

    for k in range(1, INNER):
        block_to(k).start()

    @pl.when(holder == tp)
    def _():
        own_wout.start()

    @pl.when(holder != tp)
    def _():
        mate_wout.start()

    def head(c, q):
        h = c * per_slab + q
        at = slice(q * dim, (q + 1) * dim)
        gamma = jnp.where(tp == 0, F32(decay(h, HEADS)), F32(decay(heads + h, HEADS)))

        def rotated(j):
            val = qkvg[c, j, :, at].astype(F32)
            return val * cos_ref[...] + pltpu.roll(val, dim // 2, 1) * sin_ref[...]

        query = rotated(0)
        key = rotated(1) * dim ** (-0.5)
        key_ref[:, h * dim : (h + 1) * dim] = key
        value = qkvg[c, 2, :, at].astype(F32)
        value_ref[:, h * dim : (h + 1) * dim] = qkvg[c, 2, :, at]
        across = split(query).T.astype(BF16)
        for s in range(0, seqs, 2):
            wide = jnp.dot(
                across, spread[:, s * dim : (s + 2) * dim], preferred_element_type=F32
            )
            for t in range(2):
                readout[s + t : s + t + 1, :] = jnp.sum(
                    state[s + t, h] * wide[:, t * dim : (t + 1) * dim], axis=0, keepdims=True
                )
        read = gamma * readout[...] + jnp.sum(query * key, axis=-1, keepdims=True) * value
        centred = read - jnp.mean(read, axis=-1, keepdims=True)
        scaled = centred * lax.rsqrt(jnp.mean(centred * centred, axis=-1, keepdims=True) + EPS)
        gate = qkvg[c, 3, :, at].astype(F32)
        gain = gain_wide[:, h * dim : (h + 1) * dim]
        kept[c, :, at] = (scaled * gain * (gate * jax.nn.sigmoid(gate))).astype(BF16)

    mine = tp * outer + o

    def to_cores(src, dst, send, recv, j):
        core = lax.rem(tp + j // outer, 2)
        peer = lax.rem(o + lax.rem(j, outer), outer)
        return remote(src(peer), dst, send.at[j], recv.at[j], peer * INNER + i, core)

    def source_of(j):
        core = lax.rem(tp + 2 - j // outer, 2)
        return core * outer + lax.rem(o + outer - lax.rem(j, outer), outer)

    def kept_to(c, j, source):
        return to_cores(lambda p: kept.at[c], heads_in.at[c, source], cs.at[c], cr.at[c], j)

    def retain(c):
        zin[c, me] = parts[c, me]

        @pl.loop(1, n)
        def _(k):
            came = lax.rem(me + k, n)
            copy = to_owner(c, came, came)
            copy.wait_send()
            copy.wait_recv()

        for m in range(INNER):
            qkvg[c, m] = sum(zin[c, z * INNER + m].astype(F32) for z in range(outer)).astype(BF16)
        for q in range(per_slab):
            head(c, q)

        @pl.loop(1, 2 * outer)
        def _(j):
            kept_to(c, j, mine).start()

        heads_in[c, mine] = kept[c]

    large[0].wait()
    for c in range(slabs):
        retain(c)

    for k in range(1, INNER):
        block_to(k).wait_send()

    @pl.when(holder == tp)
    def _():
        own_wout.wait()

    @pl.when(holder != tp)
    def _():
        mate_wout.wait_send()

    for core in range(2):
        for s in range(span):

            @pl.when(jnp.logical_not(jnp.logical_and(core == tp, tp * span + s == i)))
            def _(core=core, s=s):
                remote(
                    wout_hbm, wo.at[core, s], outs.at[0], outr.at[core, s], me, mate
                ).wait_recv()

            wo_flat[core, :, s * block : (s + 1) * block] = wo[core, s]

    for c in range(slabs):

        @pl.loop(1, 2 * outer)
        def _(j, c=c):
            copy = kept_to(c, j, source_of(j))
            copy.wait_send()
            copy.wait_recv()

    first, second = (
        sum(
            jnp.dot(
                heads_in[c, q * outer : (q + 1) * outer].reshape(outer * seqs, WIDE),
                wo_flat[q, c * WIDE : (c + 1) * WIDE, :],
                preferred_element_type=F32,
            )
            for c in range(slabs)
        ).astype(BF16)
        for q in range(2)
    )
    mixer = (first.astype(F32) + second.astype(F32)).astype(BF16).astype(F32)

    @pl.loop(1, outer)
    def _(k):
        copy = columns_to(k, lax.rem(o + outer - k, outer))
        copy.wait_send()
        copy.wait_recv()

    residual = (xline[...].reshape(outer * seqs, kb // 2).astype(F32) + mixer).astype(BF16)
    rblock[...] = residual
    gathered[tp, me] = residual

    def along(peer, block_id):
        return remote(
            rblock, gathered.at[tp, block_id], ezs.at[peer], er.at[block_id], peer * INNER + i, tp
        )

    def inside(src, k, z, block_id):
        peer = lax.rem(i + k, INNER)
        return remote(
            src, gathered.at[tp, block_id], eps.at[z, k], er.at[block_id], o * INNER + peer, tp
        )

    def across_cores(src, half_id, block_id):
        return remote(
            src, gathered.at[half_id, block_id], ms.at[block_id], mr.at[block_id], me, mate
        )

    @pl.loop(1, outer)
    def _(d):
        on_line(outer - d, lambda peer: along(peer, me).start())

    for k in range(1, INNER):
        inside(rblock, k, o, me).start()
    across_cores(rblock, tp, me).start()

    def from_group(z):
        for j in range(1, INNER):
            came = z * INNER + lax.rem(i + INNER - j, INNER)
            inside(rblock, j, z, came).wait_recv()
            across_cores(gathered.at[tp, came], tp, came).start()

    def relay(peer):
        came = peer * INNER + i
        along(peer, came).wait_recv()
        for j in range(1, INNER):
            inside(gathered.at[tp, came], j, peer, came).start()
        across_cores(gathered.at[tp, came], tp, came).start()

    @pl.loop(1, n)
    def _(k):
        copy = share_to(k, lax.rem(me + n - k, n))
        copy.wait_send()
        copy.wait_recv()

    for j in range(n):
        table[j : j + 1, :] = shares[j]
    columns = table[...].T[:seqs]
    for j in range(n):
        at = ((j % INNER) * outer + j // INNER) * seqs
        opening[at : at + seqs, :LANES] = jnp.broadcast_to(columns[:, j : j + 1], (seqs, LANES))

    cols = eg.shape[1]
    dcols = dg.shape[1]
    tile = min(256, cols)
    wide = 2 * cols

    def chunk(z, c, first):
        got = gathered[c, pl.ds(z * INNER, INNER)].reshape(tokens, kb // 2).astype(F32)
        left = (got * nffn_wide[z, c]).astype(BF16)
        k_at = pl.ds(pl.multiple_of(z * kb + c * (kb // 2), kb // 2), kb // 2)

        def put(ref, at, value):
            if first:
                ref[:, at] = value
            else:
                ref[:, at] += value

        put(squares, slice(None), got * got)
        for base, w in ((0, eg), (cols, eu)):
            for j in range(cols // tile):
                src = slice(j * tile, (j + 1) * tile)
                dst = slice(base + j * tile, base + (j + 1) * tile)
                put(acc, dst, jnp.dot(left, w[k_at, src], preferred_element_type=F32))
        for base, w in ((wide, dg), (wide + dcols, du)):
            put(
                acc, slice(base, base + dcols),
                jnp.dot(left, w[k_at, :], preferred_element_type=F32),
            )
        put(
            acc, slice(wide + 2 * dcols, wide + 2 * dcols + LANES),
            lax.dot_general(
                left, open_rows[z, c], (((1,), (1,)), ((), ())), preferred_element_type=F32
            ),
        )

    def from_mate(z):
        for j in range(INNER):
            copy = across_cores(rblock, mate, z * INNER + j)
            copy.wait_send()
            copy.wait_recv()

    def own_part(z):
        from_group(z)
        chunk(z, tp, False)

    def mate_part(z):
        from_mate(z)
        chunk(z, mate, False)

    @pl.loop(1, outer)
    def _(d):
        on_line(d, relay)

    for copy in large[1:]:
        copy.wait()

    from_group(o)
    chunk(o, tp, True)
    on_line(1, own_part)
    mate_part(o)

    @pl.loop(2, outer)
    def _(d):
        on_line(d, own_part)
        on_line(d - 1, mate_part)

    on_line(outer - 1, mate_part)

    mean = jnp.sum(squares[...], axis=-1, keepdims=True) * (1.0 / width)
    scales[...] = jnp.broadcast_to(lax.rsqrt(mean + EPS), (tokens, LANES))
    opening[:, LANES:] = jax.nn.sigmoid(
        scales[...] * acc[:, wide + 2 * dcols : wide + 2 * dcols + LANES]
    )
    scale = scales[:, :1]

    @pl.loop(0, cols // tile)
    def _(j):
        at = pl.ds(pl.multiple_of(j * tile, tile), tile)
        gate = scale * acc[:, at]
        up = scale * acc[:, pl.ds(pl.multiple_of(cols + j * tile, tile), tile)]
        hidden[:, at] = (gate * jax.nn.sigmoid(gate) * up).astype(BF16)

    gate = scale * acc[:, wide : wide + dcols]
    dense_hidden[...] = (
        gate * jax.nn.sigmoid(gate) * (scale * acc[:, wide + dcols : wide + 2 * dcols])
    ).astype(BF16)

    piece = half // CHUNKS
    step = min(256, piece)

    def branch(at):
        expert_part = jnp.dot(hidden[...], ed[:, at], preferred_element_type=F32)
        dense_part = jnp.dot(dense_hidden[...], dd[:, at], preferred_element_type=F32)
        return expert_part * opening[:, :1] + dense_part * opening[:, LANES : LANES + 1]

    def swap(c):
        return remote(other.at[c], other_in.at[c], sws.at[c], swr.at[c], me, mate)

    for c in range(CHUNKS):

        @pl.loop(0, piece // step)
        def _(j, c=c):
            src = pl.ds(pl.multiple_of(mate * half + c * piece + j * step, step), step)
            other[c, :, pl.ds(pl.multiple_of(j * step, step), step)] = branch(src).astype(BF16)

        swap(c).start()

    def in_group(c, z, k, source):
        peer = lax.rem(i + k, INNER)
        return remote(
            summed.at[c, peer, z], plane_in.at[c, z, source], f1s.at[c, z, k], f1r.at[c, z, k],
            o * INNER + peer, tp,
        )

    def in_line(c, peer, source):
        return remote(
            line_out.at[c, peer], line_in.at[c, source], f2s.at[c, peer], f2r.at[c, source],
            peer * INNER + i, tp,
        )

    def send_group(c, z):
        for j in range(1, INNER):
            in_group(c, z, j, i).start()

    for c in range(CHUNKS):
        mine_at = pl.multiple_of(tp * half + c * piece, piece)
        for j in range(piece // step):
            own[:, j * step : (j + 1) * step] = branch(pl.ds(mine_at + j * step, step))
        swap(c).wait()
        for j in range(piece // step):
            at = slice(j * step, (j + 1) * step)
            both = own[:, at] + other_in[c, :, at].astype(F32)
            summed[c, :, :, :, at] = both.astype(BF16).reshape(INNER, outer, seqs, step)

        @pl.loop(1, outer)
        def _(d, c=c):
            on_line(outer - d, functools.partial(send_group, c))

    for c in range(CHUNKS):
        send_group(c, o)

    @pl.loop(1, outer)
    def _(d):
        on_line(d, lambda peer: along(peer, me).wait_send())

    @pl.loop(0, outer)
    def _(z):
        for j in range(1, INNER):
            inside(rblock, j, z, me).wait_send()

    for z in range(outer):
        for c in range(2):
            row[:, z * kb + c * (kb // 2) : z * kb + (c + 1) * (kb // 2)] = gathered[
                c, z * INNER + i, pl.ds(pl.multiple_of(o * seqs, seqs), seqs), :
            ].astype(F32)

    def reduce_group(c, z):
        got = summed[c, i, z].astype(F32)
        for j in range(1, INNER):
            source = lax.rem(i + INNER - j, INNER)
            copy = in_group(c, z, j, source)
            copy.wait_send()
            copy.wait_recv()
            got = got + plane_in[c, z, source].astype(F32)
        line_out[c, z] = got.astype(BF16)

    def reduce_far(c, z):
        reduce_group(c, z)
        in_line(c, z, o).start()

    for c in range(CHUNKS):

        @pl.loop(1, outer)
        def _(d, c=c):
            on_line(outer - d, functools.partial(reduce_far, c))

    for c in range(CHUNKS):
        reduce_group(c, o)

    for c in range(CHUNKS):
        line_in[c, o] = line_out[c, o]

        @pl.loop(1, outer)
        def _(k, c=c):
            peer = lax.rem(o + k, outer)
            copy = in_line(c, peer, peer)
            copy.wait_send()
            copy.wait_recv()

        got = lax.fori_loop(
            0, outer, lambda z, carry, c=c: carry + line_in[c, z].astype(F32),
            jnp.zeros((seqs, piece), F32),
        )
        kept_row = row[:, pl.ds(pl.multiple_of(tp * half + c * piece, piece), piece)]
        final[:, c * piece : (c + 1) * piece] = (kept_row + got).astype(BF16)

    last = remote(final, final_in, fs, fr, me, mate)
    last.start()
    out_ref[:, pl.ds(pl.multiple_of(tp * half, half), half)] = final[...]
    last.wait()
    out_ref[:, pl.ds(pl.multiple_of(mate * half, half), half)] = final_in[...]


def layer(n, args):
    x, pos, freq, ids, weight, nmix, nffn, opened, gain, state = args[:10]
    wq, wout, eg, ed, dg, dd = args[10], args[14], args[15], args[17], args[18], args[20]
    seqs, width = x.shape
    heads, dim = state.shape[1], state.shape[2]
    hw, block, half, tokens = heads * dim, width // n, width // 2, n * seqs
    outer = n // INNER
    span, group, kb, piece = INNER // 2, INNER * seqs, INNER * block, half // CHUNKS
    slabs = hw // WIDE
    cols, dcols = eg.shape[2], dg.shape[1]
    vm, sem = pltpu.VMEM, pltpu.SemaphoreType.DMA
    vmem = pl.BlockSpec(memory_space=pltpu.VMEM)
    hbm = pl.BlockSpec(memory_space=pltpu.HBM)
    return pl.pallas_call(
        functools.partial(layer_kernel, n, heads, dim),
        out_shape=(
            jax.ShapeDtypeStruct((seqs, width), BF16),
            jax.ShapeDtypeStruct((seqs, hw), F32),
            jax.ShapeDtypeStruct((seqs, hw), BF16),
        ),
        in_specs=[hbm] * len(args),
        out_specs=(vmem, vmem, vmem),
        scratch_shapes=[
            vm(x.shape, BF16), pltpu.SMEM(pos.shape, jnp.int32), vm(freq.shape, F32),
            vm(ids.shape, jnp.int32), vm(weight.shape, BF16), vm(nmix.shape, BF16),
            vm(nffn.shape, BF16), vm(opened.shape, BF16), vm(gain.shape, BF16),
            vm(state.shape, F32), vm(eg.shape[1:], BF16), vm(eg.shape[1:], BF16),
            vm(ed.shape[1:], BF16), vm(dg.shape, BF16), vm(dg.shape, BF16), vm(dd.shape, BF16),
            vm((outer, 2, seqs, kb // 2), BF16),
            vm((2, n, seqs, kb // 2), BF16),
            vm((PIECES * seqs, seqs * dim), BF16),
            vm((slabs, INNER, block, WIDE), BF16),
            vm((2, span, hw, block), BF16),
            vm((2, hw, span * block), BF16),
            vm((slabs, n, seqs, WIDE), BF16),
            vm((slabs, n, seqs, WIDE), BF16),
            vm((slabs, INNER, seqs, WIDE), BF16),
            vm((1, hw), F32),
            vm((LANES, LANES), F32),
            vm((n, 1, LANES), F32),
            vm((n, 1, LANES), F32),
            vm((seqs, dim), F32), vm((seqs, dim), F32), vm((seqs, dim), F32),
            vm((slabs, seqs, WIDE), BF16),
            vm((slabs, 2 * outer, seqs, WIDE), BF16),
            vm((outer, 2, seqs, kb // 2), BF16),
            vm((outer, seqs, kb // 2), BF16),
            vm((outer * seqs, kb // 2), BF16),
            vm((seqs, width), F32),
            vm((2, n, outer * seqs, kb // 2), BF16),
            vm((outer, 2, 1, kb // 2), F32),
            vm((outer, 2, LANES, kb // 2), BF16),
            vm((tokens, kb // 2), F32),
            vm((tokens, LANES), F32),
            vm((tokens, 2 * cols + 2 * dcols + LANES), F32),
            vm((tokens, cols), BF16),
            vm((tokens, dcols), BF16),
            vm((tokens, 2 * LANES), F32),
            vm((CHUNKS, tokens, piece), BF16),
            vm((CHUNKS, tokens, piece), BF16),
            vm((tokens, piece), F32),
            vm((CHUNKS, INNER, outer, seqs, piece), BF16),
            vm((CHUNKS, outer, INNER, seqs, piece), BF16),
            vm((CHUNKS, outer, seqs, piece), BF16),
            vm((CHUNKS, outer, seqs, piece), BF16),
            vm((seqs, half), BF16),
            vm((seqs, half), BF16),
            sem((16,)),
            sem((n,)), sem((n,)), sem((2,)),
            sem((slabs, INNER)), sem((slabs, INNER)), sem((slabs + 1,)),
            sem((INNER,)), sem((2, span)),
            sem((n,)), sem((n,)),
            sem((slabs, n)), sem((slabs, n)),
            sem((slabs, 2 * outer)), sem((slabs, 2 * outer)),
            sem((outer,)), sem((outer,)),
            sem((outer,)), sem((outer, INNER)), sem((n,)),
            sem((n,)), sem((n,)),
            sem((CHUNKS,)), sem((CHUNKS,)),
            sem((CHUNKS, outer, INNER)), sem((CHUNKS, outer, INNER)),
            sem((CHUNKS, outer)), sem((CHUNKS, outer)),
            sem, sem,
        ],
        compiler_params=pltpu.CompilerParams(
            collective_id=0, has_side_effects=True, vmem_limit_bytes=60 * 2**20
        ),
        name="layer",
    )(*args)


def update_kernel(heads, out_in, key_ref, value_ref, state_ref, out_ref, new_ref):
    seqs = key_ref.shape[0]
    dim = value_ref.shape[1] // heads
    tp = lax.axis_index("tp")

    @pl.when(pl.program_id(0) == 0)
    def _():
        out_ref[...] = out_in[...]

    row = lax.broadcasted_iota(jnp.int32, (seqs, 2 * dim), 0)
    lane = lax.broadcasted_iota(jnp.int32, (seqs, 2 * dim), 1) // dim
    for h in range(heads):
        gamma = jnp.where(tp == 0, F32(decay(h, HEADS)), F32(decay(heads + h, HEADS)))
        at = slice(h * dim, (h + 1) * dim)
        key = split(key_ref[:, at]).T.astype(BF16)
        value = value_ref[:, at].astype(F32)
        twice = jnp.concatenate([value, value], axis=1)
        for s in range(0, seqs, 2):
            spread = jnp.where(row == s + lane, twice, 0.0)
            spread = jnp.concatenate([spread] * PIECES, axis=0).astype(BF16)
            added = jnp.dot(key, spread, preferred_element_type=F32)
            for t in range(2):
                new_ref[s + t, h] = gamma * state_ref[s + t, h] + added[:, t * dim : (t + 1) * dim]


def update(out, key, value, state):
    seqs, heads, dim = state.shape[:3]
    few = min(8, seqs)
    held = pl.BlockSpec((few, heads, dim, dim), lambda j: (j, 0, 0, 0))
    piece = pl.BlockSpec((few, heads * dim), lambda j: (j, 0))
    whole = pl.BlockSpec(out.shape, lambda j: (0, 0))
    return pl.pallas_call(
        functools.partial(update_kernel, heads),
        grid=(seqs // few,),
        out_shape=(
            jax.ShapeDtypeStruct(out.shape, BF16),
            jax.ShapeDtypeStruct(state.shape, F32),
        ),
        in_specs=[whole, piece, piece, held],
        out_specs=(whole, held),
        compiler_params=pltpu.CompilerParams(vmem_limit_bytes=60 * 2**20),
        name="update",
    )(out, key, value, state)


def on_device(
    inputs,
    positions,
    ret_state,
    norm_mix,
    w_query,
    w_key,
    w_value,
    w_gate_in,
    head_gain,
    w_out,
    norm_ffn,
    route_ids,
    route_weight,
    exp_gate,
    exp_up,
    exp_down,
    dense_gate,
    dense_up,
    dense_down,
    branch_gate,
):
    n = lax.axis_size("ep")
    dim = ret_state.shape[2]
    assert exp_gate.shape[0] == 1 and n % (2 * INNER) == 0 and n <= LANES
    assert w_query.shape[1] % WIDE == 0 and WIDE % dim == 0
    turns = 10000.0 ** (-2.0 * np.arange(dim // 2) / dim)
    freq = jnp.asarray(np.concatenate([turns, turns])[None].astype(np.float32))
    out, key, value = layer(
        n,
        (inputs, positions, freq, route_ids.T, route_weight.T, norm_mix, norm_ffn, branch_gate,
         head_gain, ret_state, w_query, w_key, w_value, w_gate_in, w_out, exp_gate, exp_up,
         exp_down, dense_gate, dense_up, dense_down),
    )
    return update(out, key, value, ret_state)


def solution(mesh):
    in_specs = (
        P("ep", None),
        P("ep"),
        P("ep", "tp", None, None),
        P(),
        P("ep", "tp"),
        P("ep", "tp"),
        P("ep", "tp"),
        P("ep", "tp"),
        P("tp"),
        P("tp", "ep"),
        P(),
        P("ep", None),
        P("ep", None),
        P("ep", None, "tp"),
        P("ep", None, "tp"),
        P("ep", "tp", None),
        P(None, ("ep", "tp")),
        P(None, ("ep", "tp")),
        P(("ep", "tp"), None),
        P(),
    )
    out_specs = (P("ep", None), P("ep", "tp", None, None))
    return jax.shard_map(
        on_device, mesh=mesh, in_specs=in_specs, out_specs=out_specs, check_vma=False
    )
```

```python
import functools
import math

import jax
import jax.numpy as jnp
import numpy as np
from jax import lax
from jax.experimental import pallas as pl
from jax.experimental.pallas import tpu as pltpu
from jax.sharding import PartitionSpec as P

HEADS = 12
EPS = 1e-06
MESH = pl.DeviceIdType.MESH
LANES = 128
F32 = jnp.float32
BF16 = jnp.bfloat16
INNER = 4
CHUNKS = 2
WIDE = 384
PIECES = 3


def decay(head, head_count):
    return 1.0 - 2.0 ** (-5.0 - 5.0 * head / max(head_count - 1, 1))


def normalize(values, gain):
    return (values * lax.rsqrt(jnp.mean(values * values, axis=-1, keepdims=True) + EPS) * gain).astype(
        BF16
    )


def split(values):
    rest, pieces = values, []
    for _ in range(PIECES):
        pieces.append(rest.astype(BF16).astype(F32))
        rest = rest - pieces[-1]
    return jnp.concatenate(pieces, axis=0)


def remote(src, dst, send, recv, ep, tp):
    return pltpu.make_async_remote_copy(
        src_ref=src,
        dst_ref=dst,
        send_sem=send,
        recv_sem=recv,
        device_id=(ep, tp),
        device_id_type=MESH,
    )


def layer_kernel(
    n, heads, dim,
    x_hbm, pos_hbm, freq_hbm, ids_hbm, weight_hbm, nmix_hbm, nffn_hbm, open_hbm, gain_hbm,
    state_hbm, wq, wk, wv, wg, wout_hbm, eg_hbm, eu_hbm, ed_hbm, dg_hbm, du_hbm, dd_hbm,
    packed,
    x_ref, pos_ref, freq_ref, ids_ref, weight_ref, nmix_ref, nffn_ref, open_ref, gain_ref,
    state, eg, eu, ed, dg, du, dd,
    xsend, xrows, spread, wcol, wo, wo_flat, parts, zin, qkvg,
    gain_wide, table, share_rows, shares, cos_ref, sin_ref, readout, kept, heads_in,
    raw, xline, rblock, row, gathered, nffn_wide, open_rows, squares, scales, acc, hidden, hidden_in, dense_hidden, dense_in, opening,
    own, summed, plane_in, line_out, line_in, final, final_in,
    load, xs, xr, xm, ws, wr, local, outs, outr, shs, shr, zs, zr, cs, cr, xls, xlr,
    ezs, eps, er, ms, mr, sws, swr, f1s, f1r, f2s, f2r, fs, fr, across_send, across_recv,
):
    me, tp = lax.axis_index("ep"), lax.axis_index("tp")
    mate = 1 - tp
    outer = n // INNER
    span = INNER // 2
    o, i = me // INNER, lax.rem(me, INNER)
    seqs, width = x_ref.shape
    block, half, tokens, group = width // n, width // 2, n * seqs, INNER * seqs
    kb = INNER * block
    hw = heads * dim
    slabs, per_slab = hw // WIDE, WIDE // dim

    def half_at(c):
        return pl.ds(pl.multiple_of(c * half, half), half)

    rows_across = [
        remote(src, dst, across_send.at[j], across_recv.at[j], me, mate)
        for j, (src, dst) in enumerate(
            ((ed_hbm.at[0, :, half_at(mate)], ed.at[tp]), (dd_hbm.at[:, half_at(mate)], dd.at[tp]))
        )
    ]
    rows_here = [
        remote(src, dst, across_send.at[j], across_recv.at[j], me, mate)
        for j, (src, dst) in enumerate(
            ((ed_hbm.at[0, :, half_at(mate)], ed.at[mate]),
             (dd_hbm.at[:, half_at(mate)], dd.at[mate]))
        )
    ]

    small = [
        pltpu.make_async_copy(src, dst, load.at[j])
        for j, (src, dst) in enumerate(
            ((x_hbm, x_ref), (nmix_hbm, nmix_ref), (ids_hbm, ids_ref), (weight_hbm, weight_ref),
             (pos_hbm, pos_ref), (freq_hbm, freq_ref), (nffn_hbm, nffn_ref), (open_hbm, open_ref),
             (gain_hbm, gain_ref))
        )
    ]
    large = [
        pltpu.make_async_copy(src, dst, load.at[len(small) + j])
        for j, (src, dst) in enumerate(
            ((state_hbm, state), (eg_hbm.at[0], eg), (eu_hbm.at[0], eu), (dg_hbm, dg),
             (du_hbm, du), (ed_hbm.at[0, :, half_at(tp)], ed.at[tp]),
             (dd_hbm.at[:, half_at(tp)], dd.at[tp]))
        )
    ]
    for copy in small:
        copy.start()

    def on_line(far, act):
        for sign in (1, -1):
            peer = o + sign * far

            @pl.when(jnp.logical_and(peer >= 0, peer < outer))
            def _(peer=peer):
                act(peer)

    barrier = pltpu.get_barrier_semaphore()

    def greet(ep, core):
        pl.semaphore_signal(barrier, inc=1, device_id=(ep, core), device_id_type=MESH)

    @pl.loop(1, n)
    def _(k):
        greet(lax.rem(me + k, n), tp)

    for j in range(INNER):
        greet(o * INNER + j, mate)

    @pl.loop(1, outer)
    def _(k):
        greet(lax.rem(o + k, outer) * INNER + i, mate)

    small[0].wait()
    small[1].wait()
    normed = normalize(x_ref[...].astype(F32), nmix_ref[...].astype(F32).reshape(1, width))
    for z in range(outer):
        for c in range(2):
            at = slice(z * kb + c * (kb // 2), z * kb + (c + 1) * (kb // 2))
            xsend[z, c] = normed[:, at]
            raw[z, c] = x_ref[:, at]
    pl.semaphore_wait(barrier, n - 1 + INNER + outer - 1)

    @pl.loop(1, n)
    def _(k):
        peer = lax.rem(me + k, n)
        remote(
            xsend.at[peer // INNER, tp], xrows.at[tp, me], xs.at[k], xr.at[k], peer, tp
        ).start()

    def rows_of(c, m, w, source):
        return remote(
            w.at[:, c * WIDE : (c + 1) * WIDE], wcol.at[c, source], ws.at[c, m], wr.at[c, source],
            o * INNER + m, tp,
        )

    def own_rows(c, m, w):
        return pltpu.make_async_copy(w.at[:, c * WIDE : (c + 1) * WIDE], wcol.at[c, m], local.at[c])

    for c in range(slabs):
        for m, w in enumerate((wq, wk, wv, wg)):

            @pl.when(i != m)
            def _(c=c, m=m, w=w):
                rows_of(c, m, w, i).start()

            @pl.when(i == m)
            def _(c=c, m=m, w=w):
                own_rows(c, m, w).start()

    holder, slot = i // span, lax.rem(i, span)

    def block_to(k):
        peer = lax.rem(i + k, INNER)
        return remote(
            wout_hbm, wo.at[tp, slot], outs.at[k], outr.at[tp, slot], o * INNER + peer, holder
        )

    own_wout = pltpu.make_async_copy(wout_hbm, wo.at[tp, slot], local.at[slabs])
    mate_wout = remote(wout_hbm, wo.at[tp, slot], outs.at[0], outr.at[tp, slot], me, mate)

    def columns_to(k, source):
        peer = lax.rem(o + k, outer)
        return remote(
            raw.at[peer, tp], xline.at[source], xls.at[k], xlr.at[k], peer * INNER + i, tp
        )

    @pl.loop(1, outer)
    def _(k):
        columns_to(k, o).start()

    xline[o] = raw[o, tp]
    for copy in large:
        copy.start()
    xrows[tp, me] = xsend[o, tp]

    for j in (2, 3, 4, 5, 6, 7, 8):
        small[j].wait()
    widened = weight_ref[...].astype(F32)
    part = widened / jnp.sum(widened, axis=0, keepdims=True)
    expert = lax.broadcasted_iota(jnp.int32, (n, seqs), 0)
    named = jnp.zeros((n, seqs), F32)
    for j in range(ids_ref.shape[0]):
        named = named + jnp.where(ids_ref[j : j + 1, :] == expert, part[j : j + 1, :], 0.0)
    table[...] = jnp.zeros_like(table)
    table[:n, :seqs] = named
    for j in range(n):
        share_rows[j] = table[j : j + 1, :]

    def share_to(k, source):
        peer = lax.rem(me + k, n)
        return remote(share_rows.at[peer], shares.at[source], shs.at[k], shr.at[k], peer, tp)

    @pl.loop(1, n)
    def _(k):
        share_to(k, me).start()

    shares[me] = share_rows[me]

    rows_at = lax.broadcasted_iota(jnp.int32, (seqs, dim), 0)
    place = jnp.zeros((seqs, dim), F32)
    for s in range(seqs):
        place = jnp.where(rows_at == s, pos_ref[s].astype(F32), place)
    angles = place * freq_ref[...]
    lower = lax.broadcasted_iota(jnp.int32, (seqs, dim), 1) < dim // 2
    cos_ref[...] = jnp.cos(angles)
    sine = jnp.sin(angles)
    sin_ref[...] = jnp.where(lower, -sine, sine)
    gains = nffn_ref[...].astype(F32).reshape(1, width)
    opens = open_ref[...].astype(F32).reshape(1, width)
    for z in range(outer):
        for c in range(2):
            at = slice(z * kb + c * (kb // 2), z * kb + (c + 1) * (kb // 2))
            nffn_wide[z, c] = gains[:, at]
            open_rows[z, c] = jnp.broadcast_to(opens[:, at], (LANES, kb // 2)).astype(BF16)
    apart = lax.rem(lax.broadcasted_iota(jnp.int32, spread.shape, 0), seqs)
    spread[...] = jnp.where(
        apart == lax.broadcasted_iota(jnp.int32, spread.shape, 1) // dim, 1.0, 0.0
    ).astype(BF16)
    gain_wide[...] = gain_ref[...].astype(F32).reshape(1, hw)

    @pl.loop(1, n)
    def _(k):
        peer, came = lax.rem(me + k, n), lax.rem(me + n - k, n)
        copy = remote(
            xsend.at[peer // INNER, tp], xrows.at[tp, came], xs.at[k], xr.at[k], peer, tp
        )
        copy.wait_send()
        copy.wait_recv()

    def rows_to_mate(c):
        return remote(xrows.at[tp], xrows.at[c], xm.at[0], xm.at[1], me, mate)

    rows_to_mate(tp).start()

    def to_owner(c, peer, source):
        return remote(
            parts.at[c, peer], zin.at[c, source], zs.at[c, peer], zr.at[c, source], peer, tp
        )

    def scatter(c):
        @pl.loop(1, outer)
        def _(d):
            def send(z):
                for j in range(INNER):
                    to_owner(c, z * INNER + j, me).start()

            on_line(outer - d, send)

        for k in range(1, INNER):
            to_owner(c, o * INNER + lax.rem(i + k, INNER), me).start()

    for c in range(slabs):
        for m, w in enumerate((wq, wk, wv, wg)):

            @pl.when(i != m)
            def _(c=c, m=m, w=w):
                copy = rows_of(c, m, w, m)
                copy.wait_send()
                copy.wait_recv()

            @pl.when(i == m)
            def _(c=c, m=m, w=w):
                own_rows(c, m, w).wait()

        if c == 0:
            swapped = rows_to_mate(mate)
            swapped.wait_send()
            swapped.wait_recv()
        product = sum(
            jnp.dot(
                xrows[q].reshape(tokens, kb // 2),
                wcol[c, q * 2 : q * 2 + 2].reshape(kb // 2, WIDE),
                preferred_element_type=F32,
            )
            for q in range(2)
        )
        parts[c] = product.astype(BF16).reshape(n, seqs, WIDE)
        scatter(c)

    for k in range(1, INNER):
        block_to(k).start()

    @pl.when(holder == tp)
    def _():
        own_wout.start()

    @pl.when(holder != tp)
    def _():
        mate_wout.start()

    def head(c, q):
        h = c * per_slab + q
        at = slice(q * dim, (q + 1) * dim)
        gamma = jnp.where(tp == 0, F32(decay(h, HEADS)), F32(decay(heads + h, HEADS)))

        def rotated(j):
            val = qkvg[c, j, :, at].astype(F32)
            return val * cos_ref[...] + pltpu.roll(val, dim // 2, 1) * sin_ref[...]

        query = rotated(0)
        key = rotated(1) * dim ** (-0.5)
        packed[:, width + h * dim : width + (h + 1) * dim] = key
        value = qkvg[c, 2, :, at].astype(F32)
        packed[:, width + hw + h * dim : width + hw + (h + 1) * dim] = value
        across = split(query).T.astype(BF16)
        for s in range(0, seqs, 2):
            wide = jnp.dot(
                across, spread[:, s * dim : (s + 2) * dim], preferred_element_type=F32
            )
            for t in range(2):
                readout[s + t : s + t + 1, :] = jnp.sum(
                    state[s + t, h] * wide[:, t * dim : (t + 1) * dim], axis=0, keepdims=True
                )
        read = gamma * readout[...] + jnp.sum(query * key, axis=-1, keepdims=True) * value
        centred = read - jnp.mean(read, axis=-1, keepdims=True)
        scaled = centred * lax.rsqrt(jnp.mean(centred * centred, axis=-1, keepdims=True) + EPS)
        gate = qkvg[c, 3, :, at].astype(F32)
        gain = gain_wide[:, h * dim : (h + 1) * dim]
        kept[c, :, at] = (scaled * gain * (gate * jax.nn.sigmoid(gate))).astype(BF16)

    mine = tp * outer + o

    def to_cores(src, dst, send, recv, j):
        core = lax.rem(tp + j // outer, 2)
        peer = lax.rem(o + lax.rem(j, outer), outer)
        return remote(src(peer), dst, send.at[j], recv.at[j], peer * INNER + i, core)

    def source_of(j):
        core = lax.rem(tp + 2 - j // outer, 2)
        return core * outer + lax.rem(o + outer - lax.rem(j, outer), outer)

    def kept_to(c, j, source):
        return to_cores(lambda p: kept.at[c], heads_in.at[c, source], cs.at[c], cr.at[c], j)

    def retain(c):
        zin[c, me] = parts[c, me]

        @pl.loop(1, n)
        def _(k):
            came = lax.rem(me + k, n)
            copy = to_owner(c, came, came)
            copy.wait_send()
            copy.wait_recv()

        for m in range(INNER):
            qkvg[c, m] = sum(zin[c, z * INNER + m].astype(F32) for z in range(outer)).astype(BF16)
        for q in range(per_slab):
            head(c, q)

        @pl.loop(1, 2 * outer)
        def _(j):
            kept_to(c, j, mine).start()

        heads_in[c, mine] = kept[c]

    large[0].wait()
    for c in range(slabs):
        retain(c)

    for copy in rows_across:
        copy.start()

    for k in range(1, INNER):
        block_to(k).wait_send()

    @pl.when(holder == tp)
    def _():
        own_wout.wait()

    @pl.when(holder != tp)
    def _():
        mate_wout.wait_send()

    for core in range(2):
        for s in range(span):

            @pl.when(jnp.logical_not(jnp.logical_and(core == tp, tp * span + s == i)))
            def _(core=core, s=s):
                remote(
                    wout_hbm, wo.at[core, s], outs.at[0], outr.at[core, s], me, mate
                ).wait_recv()

            wo_flat[core, :, s * block : (s + 1) * block] = wo[core, s]

    for c in range(slabs):

        @pl.loop(1, 2 * outer)
        def _(j, c=c):
            copy = kept_to(c, j, source_of(j))
            copy.wait_send()
            copy.wait_recv()

    first, second = (
        sum(
            jnp.dot(
                heads_in[c, q * outer : (q + 1) * outer].reshape(outer * seqs, WIDE),
                wo_flat[q, c * WIDE : (c + 1) * WIDE, :],
                preferred_element_type=F32,
            )
            for c in range(slabs)
        ).astype(BF16)
        for q in range(2)
    )
    mixer = (first.astype(F32) + second.astype(F32)).astype(BF16).astype(F32)

    @pl.loop(1, outer)
    def _(k):
        copy = columns_to(k, lax.rem(o + outer - k, outer))
        copy.wait_send()
        copy.wait_recv()

    residual = (xline[...].reshape(outer * seqs, kb // 2).astype(F32) + mixer).astype(BF16)
    rblock[...] = residual
    gathered[tp, me] = residual

    def along(peer, block_id):
        return remote(
            rblock, gathered.at[tp, block_id], ezs.at[peer], er.at[block_id], peer * INNER + i, tp
        )

    def inside(src, k, z, block_id):
        peer = lax.rem(i + k, INNER)
        return remote(
            src, gathered.at[tp, block_id], eps.at[z, k], er.at[block_id], o * INNER + peer, tp
        )

    def across_cores(src, half_id, block_id):
        return remote(
            src, gathered.at[half_id, block_id], ms.at[block_id], mr.at[block_id], me, mate
        )

    @pl.loop(1, outer)
    def _(d):
        on_line(outer - d, lambda peer: along(peer, me).start())

    for k in range(1, INNER):
        inside(rblock, k, o, me).start()
    across_cores(rblock, tp, me).start()

    def from_group(z):
        for j in range(1, INNER):
            came = z * INNER + lax.rem(i + INNER - j, INNER)
            inside(rblock, j, z, came).wait_recv()
            across_cores(gathered.at[tp, came], tp, came).start()

    def relay(peer):
        came = peer * INNER + i
        along(peer, came).wait_recv()
        for j in range(1, INNER):
            inside(gathered.at[tp, came], j, peer, came).start()
        across_cores(gathered.at[tp, came], tp, came).start()

    @pl.loop(1, n)
    def _(k):
        copy = share_to(k, lax.rem(me + n - k, n))
        copy.wait_send()
        copy.wait_recv()

    for j in range(n):
        table[j : j + 1, :] = shares[j]
    columns = table[...].T[:seqs]
    for j in range(n):
        at = ((j % INNER) * outer + j // INNER) * seqs
        opening[at : at + seqs, :LANES] = jnp.broadcast_to(columns[:, j : j + 1], (seqs, LANES))

    cols = eg.shape[1]
    dcols = dg.shape[1]
    tile = min(256, cols)
    wide = 2 * cols

    def chunk(z, c, first):
        got = gathered[c, pl.ds(z * INNER, INNER)].reshape(tokens, kb // 2).astype(F32)
        left = (got * nffn_wide[z, c]).astype(BF16)
        k_at = pl.ds(pl.multiple_of(z * kb + c * (kb // 2), kb // 2), kb // 2)

        def put(ref, at, value):
            if first:
                ref[:, at] = value
            else:
                ref[:, at] += value

        put(squares, slice(None), got * got)
        for base, w in ((0, eg), (cols, eu)):
            for j in range(cols // tile):
                src = slice(j * tile, (j + 1) * tile)
                dst = slice(base + j * tile, base + (j + 1) * tile)
                put(acc, dst, jnp.dot(left, w[k_at, src], preferred_element_type=F32))
        for base, w in ((wide, dg), (wide + dcols, du)):
            put(
                acc, slice(base, base + dcols),
                jnp.dot(left, w[k_at, :], preferred_element_type=F32),
            )
        put(
            acc, slice(wide + 2 * dcols, wide + 2 * dcols + LANES),
            lax.dot_general(
                left, open_rows[z, c], (((1,), (1,)), ((), ())), preferred_element_type=F32
            ),
        )

    def from_mate(z):
        for j in range(INNER):
            copy = across_cores(rblock, mate, z * INNER + j)
            copy.wait_send()
            copy.wait_recv()

    def own_part(z):
        from_group(z)
        chunk(z, tp, False)

    def mate_part(z):
        from_mate(z)
        chunk(z, mate, False)

    @pl.loop(1, outer)
    def _(d):
        on_line(d, relay)

    for copy in large[1:]:
        copy.wait()

    from_group(o)
    chunk(o, tp, True)
    on_line(1, own_part)
    mate_part(o)

    @pl.loop(2, outer)
    def _(d):
        on_line(d, own_part)
        on_line(d - 1, mate_part)

    on_line(outer - 1, mate_part)

    mean = jnp.sum(squares[...], axis=-1, keepdims=True) * (1.0 / width)
    scales[...] = jnp.broadcast_to(lax.rsqrt(mean + EPS), (tokens, LANES))
    opening[:, LANES:] = jax.nn.sigmoid(
        scales[...] * acc[:, wide + 2 * dcols : wide + 2 * dcols + LANES]
    )
    scale = scales[:, :1]

    pieces = cols // tile

    def swap(src, dst, j):
        return remote(src, dst, sws.at[j], swr.at[j], me, mate)

    for j in range(pieces):
        gate = scale * acc[:, j * tile : (j + 1) * tile]
        up = scale * acc[:, cols + j * tile : cols + (j + 1) * tile]
        hidden[j] = (gate * jax.nn.sigmoid(gate) * up).astype(BF16)
        swap(hidden.at[j], hidden_in.at[j], j).start()

    gate = scale * acc[:, wide : wide + dcols]
    dense_hidden[...] = (
        gate * jax.nn.sigmoid(gate) * (scale * acc[:, wide + dcols : wide + 2 * dcols])
    ).astype(BF16)
    swap(dense_hidden, dense_in, pieces).start()

    piece = half // CHUNKS
    step = min(256, piece)

    def branch(units, dense_units, c, at):
        expert_part = sum(
            jnp.dot(
                units[j], ed[c, j * tile : (j + 1) * tile, at], preferred_element_type=F32
            )
            for j in range(pieces)
        )
        dense_part = jnp.dot(dense_units[...], dd[c, :, at], preferred_element_type=F32)
        return expert_part * opening[:, :1] + dense_part * opening[:, LANES : LANES + 1]

    for j in range(half // step):
        at = slice(j * step, (j + 1) * step)
        own[:, at] = branch(hidden, dense_hidden, tp, at)

    for copy in rows_here:
        copy.wait_send()
        copy.wait_recv()
    for j in range(pieces):
        swap(hidden.at[j], hidden_in.at[j], j).wait()
    swap(dense_hidden, dense_in, pieces).wait()

    def in_group(c, z, k, source):
        peer = lax.rem(i + k, INNER)
        return remote(
            summed.at[c, peer, z], plane_in.at[c, z, source], f1s.at[c, z, k], f1r.at[c, z, k],
            o * INNER + peer, tp,
        )

    def in_line(c, peer, source):
        return remote(
            line_out.at[c, peer], line_in.at[c, source], f2s.at[c, peer], f2r.at[c, source],
            peer * INNER + i, tp,
        )

    def send_group(c, z):
        for j in range(1, INNER):
            in_group(c, z, j, i).start()

    for c in range(CHUNKS):
        for j in range(piece // step):
            at = slice(j * step, (j + 1) * step)
            own_at = slice(c * piece + j * step, c * piece + (j + 1) * step)
            both = own[:, own_at] + branch(hidden_in, dense_in, mate, own_at)
            summed[c, :, :, :, at] = both.astype(BF16).reshape(INNER, outer, seqs, step)

        @pl.loop(1, outer)
        def _(d, c=c):
            on_line(outer - d, functools.partial(send_group, c))

    for c in range(CHUNKS):
        send_group(c, o)

    @pl.loop(1, outer)
    def _(d):
        on_line(d, lambda peer: along(peer, me).wait_send())

    @pl.loop(0, outer)
    def _(z):
        for j in range(1, INNER):
            inside(rblock, j, z, me).wait_send()

    for z in range(outer):
        for c in range(2):
            row[:, z * kb + c * (kb // 2) : z * kb + (c + 1) * (kb // 2)] = gathered[
                c, z * INNER + i, pl.ds(pl.multiple_of(o * seqs, seqs), seqs), :
            ].astype(F32)

    def reduce_group(c, z):
        got = summed[c, i, z].astype(F32)
        for j in range(1, INNER):
            source = lax.rem(i + INNER - j, INNER)
            copy = in_group(c, z, j, source)
            copy.wait_send()
            copy.wait_recv()
            got = got + plane_in[c, z, source].astype(F32)
        line_out[c, z] = got.astype(BF16)

    def reduce_far(c, z):
        reduce_group(c, z)
        in_line(c, z, o).start()

    for c in range(CHUNKS):

        @pl.loop(1, outer)
        def _(d, c=c):
            on_line(outer - d, functools.partial(reduce_far, c))

    for c in range(CHUNKS):
        reduce_group(c, o)

    for c in range(CHUNKS):
        line_in[c, o] = line_out[c, o]

        @pl.loop(1, outer)
        def _(k, c=c):
            peer = lax.rem(o + k, outer)
            copy = in_line(c, peer, peer)
            copy.wait_send()
            copy.wait_recv()

        got = lax.fori_loop(
            0, outer, lambda z, carry, c=c: carry + line_in[c, z].astype(F32),
            jnp.zeros((seqs, piece), F32),
        )
        kept_row = row[:, pl.ds(pl.multiple_of(tp * half + c * piece, piece), piece)]
        final[:, c * piece : (c + 1) * piece] = (kept_row + got).astype(BF16)

    last = remote(final, final_in, fs, fr, me, mate)
    last.start()
    packed[:, pl.ds(pl.multiple_of(tp * half, half), half)] = final[...].astype(F32)
    last.wait()
    packed[:, pl.ds(pl.multiple_of(mate * half, half), half)] = final_in[...].astype(F32)


def layer(n, args):
    x, pos, freq, ids, weight, nmix, nffn, opened, gain, state = args[:10]
    wq, wout, eg, ed, dg, dd = args[10], args[14], args[15], args[17], args[18], args[20]
    seqs, width = x.shape
    heads, dim = state.shape[1], state.shape[2]
    hw, block, half, tokens = heads * dim, width // n, width // 2, n * seqs
    outer = n // INNER
    span, group, kb, piece = INNER // 2, INNER * seqs, INNER * block, half // CHUNKS
    slabs = hw // WIDE
    cols, dcols = eg.shape[2], dg.shape[1]
    tile = min(256, cols)
    vm, sem = pltpu.VMEM, pltpu.SemaphoreType.DMA
    vmem = pl.BlockSpec(memory_space=pltpu.VMEM)
    hbm = pl.BlockSpec(memory_space=pltpu.HBM)
    return pl.pallas_call(
        functools.partial(layer_kernel, n, heads, dim),
        out_shape=jax.ShapeDtypeStruct((seqs, width + 2 * hw), F32),
        in_specs=[hbm] * len(args),
        out_specs=vmem,
        scratch_shapes=[
            vm(x.shape, BF16), pltpu.SMEM(pos.shape, jnp.int32), vm(freq.shape, F32),
            vm(ids.shape, jnp.int32), vm(weight.shape, BF16), vm(nmix.shape, BF16),
            vm(nffn.shape, BF16), vm(opened.shape, BF16), vm(gain.shape, BF16),
            vm(state.shape, F32), vm(eg.shape[1:], BF16), vm(eg.shape[1:], BF16),
            vm((2, eg.shape[2], half), BF16), vm(dg.shape, BF16), vm(dg.shape, BF16),
            vm((2, dg.shape[1], half), BF16),
            vm((outer, 2, seqs, kb // 2), BF16),
            vm((2, n, seqs, kb // 2), BF16),
            vm((PIECES * seqs, seqs * dim), BF16),
            vm((slabs, INNER, block, WIDE), BF16),
            vm((2, span, hw, block), BF16),
            vm((2, hw, span * block), BF16),
            vm((slabs, n, seqs, WIDE), BF16),
            vm((slabs, n, seqs, WIDE), BF16),
            vm((slabs, INNER, seqs, WIDE), BF16),
            vm((1, hw), F32),
            vm((LANES, LANES), F32),
            vm((n, 1, LANES), F32),
            vm((n, 1, LANES), F32),
            vm((seqs, dim), F32), vm((seqs, dim), F32), vm((seqs, dim), F32),
            vm((slabs, seqs, WIDE), BF16),
            vm((slabs, 2 * outer, seqs, WIDE), BF16),
            vm((outer, 2, seqs, kb // 2), BF16),
            vm((outer, seqs, kb // 2), BF16),
            vm((outer * seqs, kb // 2), BF16),
            vm((seqs, width), F32),
            vm((2, n, outer * seqs, kb // 2), BF16),
            vm((outer, 2, 1, kb // 2), F32),
            vm((outer, 2, LANES, kb // 2), BF16),
            vm((tokens, kb // 2), F32),
            vm((tokens, LANES), F32),
            vm((tokens, 2 * cols + 2 * dcols + LANES), F32),
            vm((cols // tile, tokens, tile), BF16),
            vm((cols // tile, tokens, tile), BF16),
            vm((tokens, dcols), BF16),
            vm((tokens, dcols), BF16),
            vm((tokens, 2 * LANES), F32),
            vm((tokens, half), F32),
            vm((CHUNKS, INNER, outer, seqs, piece), BF16),
            vm((CHUNKS, outer, INNER, seqs, piece), BF16),
            vm((CHUNKS, outer, seqs, piece), BF16),
            vm((CHUNKS, outer, seqs, piece), BF16),
            vm((seqs, half), BF16),
            vm((seqs, half), BF16),
            sem((16,)),
            sem((n,)), sem((n,)), sem((2,)),
            sem((slabs, INNER)), sem((slabs, INNER)), sem((slabs + 1,)),
            sem((INNER,)), sem((2, span)),
            sem((n,)), sem((n,)),
            sem((slabs, n)), sem((slabs, n)),
            sem((slabs, 2 * outer)), sem((slabs, 2 * outer)),
            sem((outer,)), sem((outer,)),
            sem((outer,)), sem((outer, INNER)), sem((n,)),
            sem((n,)), sem((n,)),
            sem((cols // tile + 1,)), sem((cols // tile + 1,)),
            sem((CHUNKS, outer, INNER)), sem((CHUNKS, outer, INNER)),
            sem((CHUNKS, outer)), sem((CHUNKS, outer)),
            sem, sem, sem((2,)), sem((2,)),
        ],
        compiler_params=pltpu.CompilerParams(
            collective_id=0, has_side_effects=True, vmem_limit_bytes=56 * 2**20
        ),
        name="layer",
    )(*args)


def update_kernel(packed, state_ref, out_ref, new_ref):
    seqs, width = out_ref.shape
    heads, dim = state_ref.shape[1:3]
    hw = heads * dim
    tp = lax.axis_index("tp")
    out_ref[...] = packed[:, :width].astype(BF16)
    row = lax.broadcasted_iota(jnp.int32, (seqs, 2 * dim), 0)
    lane = lax.broadcasted_iota(jnp.int32, (seqs, 2 * dim), 1) // dim
    for h in range(heads):
        gamma = jnp.where(tp == 0, F32(decay(h, HEADS)), F32(decay(heads + h, HEADS)))
        key = packed[:, width + h * dim : width + (h + 1) * dim]
        key = split(key).T.astype(BF16)
        value = packed[:, width + hw + h * dim : width + hw + (h + 1) * dim]
        twice = jnp.concatenate([value, value], axis=1)
        for s in range(0, seqs, 2):
            spread = jnp.where(row == s + lane, twice, 0.0)
            spread = jnp.concatenate([spread] * PIECES, axis=0).astype(BF16)
            added = jnp.dot(key, spread, preferred_element_type=F32)
            for t in range(2):
                new_ref[s + t, h] = gamma * state_ref[s + t, h] + added[:, t * dim : (t + 1) * dim]


def update(packed, state):
    seqs, heads, dim = state.shape[:3]
    width = packed.shape[1] - 2 * heads * dim
    few = min(8, seqs)
    held = pl.BlockSpec((few, heads, dim, dim), lambda j: (j, 0, 0, 0))
    return pl.pallas_call(
        update_kernel,
        grid=(seqs // few,),
        out_shape=(
            jax.ShapeDtypeStruct((seqs, width), BF16),
            jax.ShapeDtypeStruct(state.shape, F32),
        ),
        in_specs=[pl.BlockSpec((few, packed.shape[1]), lambda j: (j, 0)), held],
        out_specs=(pl.BlockSpec((few, width), lambda j: (j, 0)), held),
        compiler_params=pltpu.CompilerParams(vmem_limit_bytes=16 * 2**20),
        name="update",
    )(packed, state)


def on_device(
    inputs,
    positions,
    ret_state,
    norm_mix,
    w_query,
    w_key,
    w_value,
    w_gate_in,
    head_gain,
    w_out,
    norm_ffn,
    route_ids,
    route_weight,
    exp_gate,
    exp_up,
    exp_down,
    dense_gate,
    dense_up,
    dense_down,
    branch_gate,
):
    n = lax.axis_size("ep")
    dim = ret_state.shape[2]
    assert exp_gate.shape[0] == 1 and n % (2 * INNER) == 0 and n <= LANES
    assert w_query.shape[1] % WIDE == 0 and WIDE % dim == 0
    turns = 10000.0 ** (-2.0 * np.arange(dim // 2) / dim)
    freq = jnp.asarray(np.concatenate([turns, turns])[None].astype(np.float32))
    packed = layer(
        n,
        (inputs, positions, freq, route_ids.T, route_weight.T, norm_mix, norm_ffn, branch_gate,
         head_gain, ret_state, w_query, w_key, w_value, w_gate_in, w_out, exp_gate, exp_up,
         exp_down, dense_gate, dense_up, dense_down),
    )
    return update(packed, ret_state)


def solution(mesh):
    in_specs = (
        P("ep", None),
        P("ep"),
        P("ep", "tp", None, None),
        P(),
        P("ep", "tp"),
        P("ep", "tp"),
        P("ep", "tp"),
        P("ep", "tp"),
        P("tp"),
        P("tp", "ep"),
        P(),
        P("ep", None),
        P("ep", None),
        P("ep", None, "tp"),
        P("ep", None, "tp"),
        P("ep", "tp", None),
        P(None, ("ep", "tp")),
        P(None, ("ep", "tp")),
        P(("ep", "tp"), None),
        P(),
    )
    out_specs = (P("ep", None), P("ep", "tp", None, None))
    return jax.shard_map(
        on_device, mesh=mesh, in_specs=in_specs, out_specs=out_specs, check_vma=False
    )
```

```python
import functools
import math

import jax
import jax.numpy as jnp
import numpy as np
from jax import lax
from jax.experimental import pallas as pl
from jax.experimental.pallas import tpu as pltpu
from jax.sharding import PartitionSpec as P

HEADS = 12
EPS = 1e-06
MESH = pl.DeviceIdType.MESH
LANES = 128
F32 = jnp.float32
BF16 = jnp.bfloat16
INNER = 4
CHUNKS = 2
WIDE = 384
PIECES = 3


def decay(head, head_count):
    return 1.0 - 2.0 ** (-5.0 - 5.0 * head / max(head_count - 1, 1))


def normalize(values, gain):
    return (values * lax.rsqrt(jnp.mean(values * values, axis=-1, keepdims=True) + EPS) * gain).astype(
        BF16
    )


def split(values):
    rest, pieces = values, []
    for _ in range(PIECES):
        pieces.append(rest.astype(BF16).astype(F32))
        rest = rest - pieces[-1]
    return jnp.concatenate(pieces, axis=0)


def remote(src, dst, send, recv, ep, tp):
    return pltpu.make_async_remote_copy(
        src_ref=src,
        dst_ref=dst,
        send_sem=send,
        recv_sem=recv,
        device_id=(ep, tp),
        device_id_type=MESH,
    )


def layer_kernel(
    n, heads, dim,
    x_hbm, pos_hbm, freq_hbm, ids_hbm, weight_hbm, nmix_hbm, nffn_hbm, open_hbm, gain_hbm,
    state_hbm, wq, wk, wv, wg, wout_hbm, eg_hbm, eu_hbm, ed_hbm, dg_hbm, du_hbm, dd_hbm,
    packed,
    x_ref, pos_ref, freq_ref, ids_ref, weight_ref, nmix_ref, nffn_ref, open_ref, gain_ref,
    state, eg, eu, ed, dg, du, dd,
    xsend, xrows, spread, wcol, wo, wo_flat, parts, zin, qkvg,
    gain_wide, table, share_rows, shares, cos_ref, sin_ref, readout, kept, heads_in,
    raw, xline, rblock, row, gathered, nffn_wide, open_rows, squares, scales, acc, hidden, hidden_in, dense_hidden, dense_in, opening,
    own, summed, plane_in, line_out, line_in, final, final_in,
    load, xs, xr, xm, ws, wr, local, outs, outr, shs, shr, zs, zr, cs, cr, xls, xlr,
    ezs, eps, er, ms, mr, sws, swr, f1s, f1r, f2s, f2r, fs, fr, across_send, across_recv,
):
    me, tp = lax.axis_index("ep"), lax.axis_index("tp")
    mate = 1 - tp
    outer = n // INNER
    span = INNER // 2
    o, i = me // INNER, lax.rem(me, INNER)
    seqs, width = x_ref.shape
    block, half, tokens, group = width // n, width // 2, n * seqs, INNER * seqs
    kb = INNER * block
    hw = heads * dim
    slabs, per_slab = hw // WIDE, WIDE // dim

    def half_at(c):
        return pl.ds(pl.multiple_of(c * half, half), half)

    rows_across = [
        remote(src, dst, across_send.at[j], across_recv.at[j], me, mate)
        for j, (src, dst) in enumerate(
            ((ed_hbm.at[0, :, half_at(mate)], ed.at[tp]), (dd_hbm.at[:, half_at(mate)], dd.at[tp]))
        )
    ]
    rows_here = [
        remote(src, dst, across_send.at[j], across_recv.at[j], me, mate)
        for j, (src, dst) in enumerate(
            ((ed_hbm.at[0, :, half_at(mate)], ed.at[mate]),
             (dd_hbm.at[:, half_at(mate)], dd.at[mate]))
        )
    ]

    small = [
        pltpu.make_async_copy(src, dst, load.at[j])
        for j, (src, dst) in enumerate(
            ((x_hbm, x_ref), (nmix_hbm, nmix_ref), (ids_hbm, ids_ref), (weight_hbm, weight_ref),
             (pos_hbm, pos_ref), (freq_hbm, freq_ref), (nffn_hbm, nffn_ref), (open_hbm, open_ref),
             (gain_hbm, gain_ref))
        )
    ]
    large = [
        pltpu.make_async_copy(src, dst, load.at[len(small) + j])
        for j, (src, dst) in enumerate(
            ((state_hbm, state), (eg_hbm.at[0], eg), (eu_hbm.at[0], eu), (dg_hbm, dg),
             (du_hbm, du), (ed_hbm.at[0, :, half_at(tp)], ed.at[tp]),
             (dd_hbm.at[:, half_at(tp)], dd.at[tp]))
        )
    ]
    for copy in small:
        copy.start()

    def on_line(far, act):
        for sign in (1, -1):
            peer = o + sign * far

            @pl.when(jnp.logical_and(peer >= 0, peer < outer))
            def _(peer=peer):
                act(peer)

    order = (lax.rem(INNER + 3 + 2 * INNER - 2 * i, INNER), lax.rem(INNER + 1 - 2 * lax.rem(i, 2), INNER), 2)
    barrier = pltpu.get_barrier_semaphore()

    def greet(ep, core):
        pl.semaphore_signal(barrier, inc=1, device_id=(ep, core), device_id_type=MESH)

    @pl.loop(1, n)
    def _(k):
        greet(lax.rem(me + k, n), tp)

    for j in range(INNER):
        greet(o * INNER + j, mate)

    @pl.loop(1, outer)
    def _(k):
        greet(lax.rem(o + k, outer) * INNER + i, mate)

    small[0].wait()
    small[1].wait()
    normed = normalize(x_ref[...].astype(F32), nmix_ref[...].astype(F32).reshape(1, width))
    for z in range(outer):
        for c in range(2):
            at = slice(z * kb + c * (kb // 2), z * kb + (c + 1) * (kb // 2))
            xsend[z, c] = normed[:, at]
            raw[z, c] = x_ref[:, at]
    pl.semaphore_wait(barrier, n - 1 + INNER + outer - 1)

    @pl.loop(1, n)
    def _(k):
        peer = lax.rem(me + k, n)
        remote(
            xsend.at[peer // INNER, tp], xrows.at[tp, me], xs.at[k], xr.at[k], peer, tp
        ).start()

    def rows_of(c, m, w, source):
        return remote(
            w.at[:, c * WIDE : (c + 1) * WIDE], wcol.at[c, source], ws.at[c, m], wr.at[c, source],
            o * INNER + m, tp,
        )

    def own_rows(c, m, w):
        return pltpu.make_async_copy(w.at[:, c * WIDE : (c + 1) * WIDE], wcol.at[c, m], local.at[c])

    for c in range(slabs):
        for m, w in enumerate((wq, wk, wv, wg)):

            @pl.when(i != m)
            def _(c=c, m=m, w=w):
                rows_of(c, m, w, i).start()

            @pl.when(i == m)
            def _(c=c, m=m, w=w):
                own_rows(c, m, w).start()

    holder, slot = i // span, lax.rem(i, span)

    def block_to(k):
        peer = lax.rem(i + k, INNER)
        return remote(
            wout_hbm, wo.at[tp, slot], outs.at[k], outr.at[tp, slot], o * INNER + peer, holder
        )

    own_wout = pltpu.make_async_copy(wout_hbm, wo.at[tp, slot], local.at[slabs])
    mate_wout = remote(wout_hbm, wo.at[tp, slot], outs.at[0], outr.at[tp, slot], me, mate)

    def columns_to(k, source):
        peer = lax.rem(o + k, outer)
        return remote(
            raw.at[peer, tp], xline.at[source], xls.at[k], xlr.at[k], peer * INNER + i, tp
        )

    @pl.loop(1, outer)
    def _(k):
        columns_to(k, o).start()

    xline[o] = raw[o, tp]
    for copy in large:
        copy.start()
    xrows[tp, me] = xsend[o, tp]

    for j in (2, 3, 4, 5, 6, 7, 8):
        small[j].wait()
    widened = weight_ref[...].astype(F32)
    part = widened / jnp.sum(widened, axis=0, keepdims=True)
    expert = lax.broadcasted_iota(jnp.int32, (n, seqs), 0)
    named = jnp.zeros((n, seqs), F32)
    for j in range(ids_ref.shape[0]):
        named = named + jnp.where(ids_ref[j : j + 1, :] == expert, part[j : j + 1, :], 0.0)
    table[...] = jnp.zeros_like(table)
    table[:n, :seqs] = named
    for j in range(n):
        share_rows[j] = table[j : j + 1, :]

    def share_to(k, source):
        peer = lax.rem(me + k, n)
        return remote(share_rows.at[peer], shares.at[source], shs.at[k], shr.at[k], peer, tp)

    @pl.loop(1, n)
    def _(k):
        share_to(k, me).start()

    shares[me] = share_rows[me]

    rows_at = lax.broadcasted_iota(jnp.int32, (seqs, dim), 0)
    place = jnp.zeros((seqs, dim), F32)
    for s in range(seqs):
        place = jnp.where(rows_at == s, pos_ref[s].astype(F32), place)
    angles = place * freq_ref[...]
    lower = lax.broadcasted_iota(jnp.int32, (seqs, dim), 1) < dim // 2
    cos_ref[...] = jnp.cos(angles)
    sine = jnp.sin(angles)
    sin_ref[...] = jnp.where(lower, -sine, sine)
    gains = nffn_ref[...].astype(F32).reshape(1, width)
    opens = open_ref[...].astype(F32).reshape(1, width)
    for z in range(outer):
        for c in range(2):
            at = slice(z * kb + c * (kb // 2), z * kb + (c + 1) * (kb // 2))
            nffn_wide[z, c] = gains[:, at]
            open_rows[z, c] = jnp.broadcast_to(opens[:, at], (LANES, kb // 2)).astype(BF16)
    apart = lax.rem(lax.broadcasted_iota(jnp.int32, spread.shape, 0), seqs)
    spread[...] = jnp.where(
        apart == lax.broadcasted_iota(jnp.int32, spread.shape, 1) // dim, 1.0, 0.0
    ).astype(BF16)
    gain_wide[...] = gain_ref[...].astype(F32).reshape(1, hw)

    @pl.loop(1, n)
    def _(k):
        peer, came = lax.rem(me + k, n), lax.rem(me + n - k, n)
        copy = remote(
            xsend.at[peer // INNER, tp], xrows.at[tp, came], xs.at[k], xr.at[k], peer, tp
        )
        copy.wait_send()
        copy.wait_recv()

    def rows_to_mate(c):
        return remote(xrows.at[tp], xrows.at[c], xm.at[0], xm.at[1], me, mate)

    rows_to_mate(tp).start()

    def to_owner(c, peer, source):
        return remote(
            parts.at[c, peer], zin.at[c, source], zs.at[c, peer], zr.at[c, source], peer, tp
        )

    def scatter(c):
        @pl.loop(1, outer)
        def _(d):
            def send(z):
                for j in range(INNER):
                    to_owner(c, z * INNER + j, me).start()

            on_line(outer - d, send)

        for k in range(1, INNER):
            to_owner(c, o * INNER + lax.rem(i + k, INNER), me).start()

    for c in range(slabs):
        for m, w in enumerate((wq, wk, wv, wg)):

            @pl.when(i != m)
            def _(c=c, m=m, w=w):
                copy = rows_of(c, m, w, m)
                copy.wait_send()
                copy.wait_recv()

            @pl.when(i == m)
            def _(c=c, m=m, w=w):
                own_rows(c, m, w).wait()

        if c == 0:
            swapped = rows_to_mate(mate)
            swapped.wait_send()
            swapped.wait_recv()
        product = sum(
            jnp.dot(
                xrows[q].reshape(tokens, kb // 2),
                wcol[c, q * 2 : q * 2 + 2].reshape(kb // 2, WIDE),
                preferred_element_type=F32,
            )
            for q in range(2)
        )
        parts[c] = product.astype(BF16).reshape(n, seqs, WIDE)
        scatter(c)

    for k in order:
        block_to(k).start()

    @pl.when(holder == tp)
    def _():
        own_wout.start()

    @pl.when(holder != tp)
    def _():
        mate_wout.start()

    def head(c, q):
        h = c * per_slab + q
        at = slice(q * dim, (q + 1) * dim)
        gamma = jnp.where(tp == 0, F32(decay(h, HEADS)), F32(decay(heads + h, HEADS)))

        def rotated(j):
            val = qkvg[c, j, :, at].astype(F32)
            return val * cos_ref[...] + pltpu.roll(val, dim // 2, 1) * sin_ref[...]

        query = rotated(0)
        key = rotated(1) * dim ** (-0.5)
        packed[:, width + h * dim : width + (h + 1) * dim] = key
        value = qkvg[c, 2, :, at].astype(F32)
        packed[:, width + hw + h * dim : width + hw + (h + 1) * dim] = value
        across = split(query).T.astype(BF16)
        for s in range(0, seqs, 2):
            wide = jnp.dot(
                across, spread[:, s * dim : (s + 2) * dim], preferred_element_type=F32
            )
            for t in range(2):
                readout[s + t : s + t + 1, :] = jnp.sum(
                    state[s + t, h] * wide[:, t * dim : (t + 1) * dim], axis=0, keepdims=True
                )
        read = gamma * readout[...] + jnp.sum(query * key, axis=-1, keepdims=True) * value
        centred = read - jnp.mean(read, axis=-1, keepdims=True)
        scaled = centred * lax.rsqrt(jnp.mean(centred * centred, axis=-1, keepdims=True) + EPS)
        gate = qkvg[c, 3, :, at].astype(F32)
        gain = gain_wide[:, h * dim : (h + 1) * dim]
        kept[c, :, at] = (scaled * gain * (gate * jax.nn.sigmoid(gate))).astype(BF16)

    mine = tp * outer + o

    def to_cores(src, dst, send, recv, j):
        core = lax.rem(tp + j // outer, 2)
        peer = lax.rem(o + lax.rem(j, outer), outer)
        return remote(src(peer), dst, send.at[j], recv.at[j], peer * INNER + i, core)

    def source_of(j):
        core = lax.rem(tp + 2 - j // outer, 2)
        return core * outer + lax.rem(o + outer - lax.rem(j, outer), outer)

    def kept_to(c, j, source):
        return to_cores(lambda p: kept.at[c], heads_in.at[c, source], cs.at[c], cr.at[c], j)

    def retain(c):
        zin[c, me] = parts[c, me]

        @pl.loop(1, n)
        def _(k):
            came = lax.rem(me + k, n)
            copy = to_owner(c, came, came)
            copy.wait_send()
            copy.wait_recv()

        for m in range(INNER):
            qkvg[c, m] = sum(zin[c, z * INNER + m].astype(F32) for z in range(outer)).astype(BF16)
        for q in range(per_slab):
            head(c, q)

        @pl.loop(1, 2 * outer)
        def _(j):
            kept_to(c, j, mine).start()

        heads_in[c, mine] = kept[c]

    large[0].wait()
    for c in range(slabs):
        retain(c)

    for copy in rows_across:
        copy.start()

    for k in range(1, INNER):
        block_to(k).wait_send()

    @pl.when(holder == tp)
    def _():
        own_wout.wait()

    @pl.when(holder != tp)
    def _():
        mate_wout.wait_send()

    for core in range(2):
        for s in range(span):

            @pl.when(jnp.logical_not(jnp.logical_and(core == tp, tp * span + s == i)))
            def _(core=core, s=s):
                remote(
                    wout_hbm, wo.at[core, s], outs.at[0], outr.at[core, s], me, mate
                ).wait_recv()

            wo_flat[core, :, s * block : (s + 1) * block] = wo[core, s]

    for c in range(slabs):

        @pl.loop(1, 2 * outer)
        def _(j, c=c):
            copy = kept_to(c, j, source_of(j))
            copy.wait_send()
            copy.wait_recv()

    first, second = (
        sum(
            jnp.dot(
                heads_in[c, q * outer : (q + 1) * outer].reshape(outer * seqs, WIDE),
                wo_flat[q, c * WIDE : (c + 1) * WIDE, :],
                preferred_element_type=F32,
            )
            for c in range(slabs)
        ).astype(BF16)
        for q in range(2)
    )
    mixer = (first.astype(F32) + second.astype(F32)).astype(BF16).astype(F32)

    @pl.loop(1, outer)
    def _(k):
        copy = columns_to(k, lax.rem(o + outer - k, outer))
        copy.wait_send()
        copy.wait_recv()

    residual = (xline[...].reshape(outer * seqs, kb // 2).astype(F32) + mixer).astype(BF16)
    rblock[...] = residual
    gathered[tp, me] = residual

    def along(peer, block_id):
        return remote(
            rblock, gathered.at[tp, block_id], ezs.at[peer], er.at[block_id], peer * INNER + i, tp
        )

    def inside(src, k, z, block_id):
        peer = lax.rem(i + k, INNER)
        return remote(
            src, gathered.at[tp, block_id], eps.at[z, k], er.at[block_id], o * INNER + peer, tp
        )

    def across_cores(src, half_id, block_id):
        return remote(
            src, gathered.at[half_id, block_id], ms.at[block_id], mr.at[block_id], me, mate
        )

    @pl.loop(1, outer)
    def _(d):
        on_line(outer - d, lambda peer: along(peer, me).start())

    for k in order:
        inside(rblock, k, o, me).start()
    across_cores(rblock, tp, me).start()

    def from_group(z):
        for j in range(1, INNER):
            came = z * INNER + lax.rem(i + INNER - j, INNER)
            inside(rblock, j, z, came).wait_recv()
            across_cores(gathered.at[tp, came], tp, came).start()

    def relay(peer):
        came = peer * INNER + i
        along(peer, came).wait_recv()
        for j in order:
            inside(gathered.at[tp, came], j, peer, came).start()
        across_cores(gathered.at[tp, came], tp, came).start()

    @pl.loop(1, n)
    def _(k):
        copy = share_to(k, lax.rem(me + n - k, n))
        copy.wait_send()
        copy.wait_recv()

    for j in range(n):
        table[j : j + 1, :] = shares[j]
    columns = table[...].T[:seqs]
    for j in range(n):
        at = ((j % INNER) * outer + j // INNER) * seqs
        opening[at : at + seqs, :LANES] = jnp.broadcast_to(columns[:, j : j + 1], (seqs, LANES))

    cols = eg.shape[1]
    dcols = dg.shape[1]
    tile = min(256, cols)
    wide = 2 * cols

    def chunk(z, c, first):
        got = gathered[c, pl.ds(z * INNER, INNER)].reshape(tokens, kb // 2).astype(F32)
        left = (got * nffn_wide[z, c]).astype(BF16)
        k_at = pl.ds(pl.multiple_of(z * kb + c * (kb // 2), kb // 2), kb // 2)

        def put(ref, at, value):
            if first:
                ref[:, at] = value
            else:
                ref[:, at] += value

        put(squares, slice(None), got * got)
        for base, w in ((0, eg), (cols, eu)):
            for j in range(cols // tile):
                src = slice(j * tile, (j + 1) * tile)
                dst = slice(base + j * tile, base + (j + 1) * tile)
                put(acc, dst, jnp.dot(left, w[k_at, src], preferred_element_type=F32))
        for base, w in ((wide, dg), (wide + dcols, du)):
            put(
                acc, slice(base, base + dcols),
                jnp.dot(left, w[k_at, :], preferred_element_type=F32),
            )
        put(
            acc, slice(wide + 2 * dcols, wide + 2 * dcols + LANES),
            lax.dot_general(
                left, open_rows[z, c], (((1,), (1,)), ((), ())), preferred_element_type=F32
            ),
        )

    def from_mate(z):
        for j in range(INNER):
            copy = across_cores(rblock, mate, z * INNER + j)
            copy.wait_send()
            copy.wait_recv()

    def own_part(z):
        from_group(z)
        chunk(z, tp, False)

    def mate_part(z):
        from_mate(z)
        chunk(z, mate, False)

    @pl.loop(1, outer)
    def _(d):
        on_line(d, relay)

    for copy in large[1:]:
        copy.wait()

    from_group(o)
    chunk(o, tp, True)
    on_line(1, own_part)
    mate_part(o)

    @pl.loop(2, outer)
    def _(d):
        on_line(d, own_part)
        on_line(d - 1, mate_part)

    on_line(outer - 1, mate_part)

    mean = jnp.sum(squares[...], axis=-1, keepdims=True) * (1.0 / width)
    scales[...] = jnp.broadcast_to(lax.rsqrt(mean + EPS), (tokens, LANES))
    opening[:, LANES:] = jax.nn.sigmoid(
        scales[...] * acc[:, wide + 2 * dcols : wide + 2 * dcols + LANES]
    )
    scale = scales[:, :1]

    pieces = cols // tile

    def swap(src, dst, j):
        return remote(src, dst, sws.at[j], swr.at[j], me, mate)

    for j in range(pieces):
        gate = scale * acc[:, j * tile : (j + 1) * tile]
        up = scale * acc[:, cols + j * tile : cols + (j + 1) * tile]
        hidden[j] = (gate * jax.nn.sigmoid(gate) * up).astype(BF16)
        swap(hidden.at[j], hidden_in.at[j], j).start()

    gate = scale * acc[:, wide : wide + dcols]
    dense_hidden[...] = (
        gate * jax.nn.sigmoid(gate) * (scale * acc[:, wide + dcols : wide + 2 * dcols])
    ).astype(BF16)
    swap(dense_hidden, dense_in, pieces).start()

    piece = half // CHUNKS
    step = min(256, piece)

    def branch(units, dense_units, c, at):
        expert_part = sum(
            jnp.dot(
                units[j], ed[c, j * tile : (j + 1) * tile, at], preferred_element_type=F32
            )
            for j in range(pieces)
        )
        dense_part = jnp.dot(dense_units[...], dd[c, :, at], preferred_element_type=F32)
        return expert_part * opening[:, :1] + dense_part * opening[:, LANES : LANES + 1]

    for j in range(half // step):
        at = slice(j * step, (j + 1) * step)
        own[:, at] = branch(hidden, dense_hidden, tp, at)

    for copy in rows_here:
        copy.wait_send()
        copy.wait_recv()
    for j in range(pieces):
        swap(hidden.at[j], hidden_in.at[j], j).wait()
    swap(dense_hidden, dense_in, pieces).wait()

    def in_group(c, z, k, source):
        peer = lax.rem(i + k, INNER)
        return remote(
            summed.at[c, peer, z], plane_in.at[c, z, source], f1s.at[c, z, k], f1r.at[c, z, k],
            o * INNER + peer, tp,
        )

    def in_line(c, peer, source):
        return remote(
            line_out.at[c, peer], line_in.at[c, source], f2s.at[c, peer], f2r.at[c, source],
            peer * INNER + i, tp,
        )

    def send_group(c, z):
        for j in order:
            in_group(c, z, j, i).start()

    for c in range(CHUNKS):
        for j in range(piece // step):
            at = slice(j * step, (j + 1) * step)
            own_at = slice(c * piece + j * step, c * piece + (j + 1) * step)
            both = own[:, own_at] + branch(hidden_in, dense_in, mate, own_at)
            summed[c, :, :, :, at] = both.astype(BF16).reshape(INNER, outer, seqs, step)

        @pl.loop(1, outer)
        def _(d, c=c):
            on_line(outer - d, functools.partial(send_group, c))

    for c in range(CHUNKS):
        send_group(c, o)

    @pl.loop(1, outer)
    def _(d):
        on_line(d, lambda peer: along(peer, me).wait_send())

    @pl.loop(0, outer)
    def _(z):
        for j in range(1, INNER):
            inside(rblock, j, z, me).wait_send()

    for z in range(outer):
        for c in range(2):
            row[:, z * kb + c * (kb // 2) : z * kb + (c + 1) * (kb // 2)] = gathered[
                c, z * INNER + i, pl.ds(pl.multiple_of(o * seqs, seqs), seqs), :
            ].astype(F32)

    def reduce_group(c, z):
        got = summed[c, i, z].astype(F32)
        for j in range(1, INNER):
            source = lax.rem(i + INNER - j, INNER)
            copy = in_group(c, z, j, source)
            copy.wait_send()
            copy.wait_recv()
            got = got + plane_in[c, z, source].astype(F32)
        line_out[c, z] = got.astype(BF16)

    def reduce_far(c, z):
        reduce_group(c, z)
        in_line(c, z, o).start()

    for c in range(CHUNKS):

        @pl.loop(1, outer)
        def _(d, c=c):
            on_line(outer - d, functools.partial(reduce_far, c))

    for c in range(CHUNKS):
        reduce_group(c, o)

    for c in range(CHUNKS):
        line_in[c, o] = line_out[c, o]

        @pl.loop(1, outer)
        def _(k, c=c):
            peer = lax.rem(o + k, outer)
            copy = in_line(c, peer, peer)
            copy.wait_send()
            copy.wait_recv()

        got = lax.fori_loop(
            0, outer, lambda z, carry, c=c: carry + line_in[c, z].astype(F32),
            jnp.zeros((seqs, piece), F32),
        )
        kept_row = row[:, pl.ds(pl.multiple_of(tp * half + c * piece, piece), piece)]
        final[:, c * piece : (c + 1) * piece] = (kept_row + got).astype(BF16)

    last = remote(final, final_in, fs, fr, me, mate)
    last.start()
    packed[:, pl.ds(pl.multiple_of(tp * half, half), half)] = final[...].astype(F32)
    last.wait()
    packed[:, pl.ds(pl.multiple_of(mate * half, half), half)] = final_in[...].astype(F32)


def layer(n, args):
    x, pos, freq, ids, weight, nmix, nffn, opened, gain, state = args[:10]
    wq, wout, eg, ed, dg, dd = args[10], args[14], args[15], args[17], args[18], args[20]
    seqs, width = x.shape
    heads, dim = state.shape[1], state.shape[2]
    hw, block, half, tokens = heads * dim, width // n, width // 2, n * seqs
    outer = n // INNER
    span, group, kb, piece = INNER // 2, INNER * seqs, INNER * block, half // CHUNKS
    slabs = hw // WIDE
    cols, dcols = eg.shape[2], dg.shape[1]
    tile = min(256, cols)
    vm, sem = pltpu.VMEM, pltpu.SemaphoreType.DMA
    vmem = pl.BlockSpec(memory_space=pltpu.VMEM)
    hbm = pl.BlockSpec(memory_space=pltpu.HBM)
    return pl.pallas_call(
        functools.partial(layer_kernel, n, heads, dim),
        out_shape=jax.ShapeDtypeStruct((seqs, width + 2 * hw), F32),
        in_specs=[hbm] * len(args),
        out_specs=vmem,
        scratch_shapes=[
            vm(x.shape, BF16), pltpu.SMEM(pos.shape, jnp.int32), vm(freq.shape, F32),
            vm(ids.shape, jnp.int32), vm(weight.shape, BF16), vm(nmix.shape, BF16),
            vm(nffn.shape, BF16), vm(opened.shape, BF16), vm(gain.shape, BF16),
            vm(state.shape, F32), vm(eg.shape[1:], BF16), vm(eg.shape[1:], BF16),
            vm((2, eg.shape[2], half), BF16), vm(dg.shape, BF16), vm(dg.shape, BF16),
            vm((2, dg.shape[1], half), BF16),
            vm((outer, 2, seqs, kb // 2), BF16),
            vm((2, n, seqs, kb // 2), BF16),
            vm((PIECES * seqs, seqs * dim), BF16),
            vm((slabs, INNER, block, WIDE), BF16),
            vm((2, span, hw, block), BF16),
            vm((2, hw, span * block), BF16),
            vm((slabs, n, seqs, WIDE), BF16),
            vm((slabs, n, seqs, WIDE), BF16),
            vm((slabs, INNER, seqs, WIDE), BF16),
            vm((1, hw), F32),
            vm((LANES, LANES), F32),
            vm((n, 1, LANES), F32),
            vm((n, 1, LANES), F32),
            vm((seqs, dim), F32), vm((seqs, dim), F32), vm((seqs, dim), F32),
            vm((slabs, seqs, WIDE), BF16),
            vm((slabs, 2 * outer, seqs, WIDE), BF16),
            vm((outer, 2, seqs, kb // 2), BF16),
            vm((outer, seqs, kb // 2), BF16),
            vm((outer * seqs, kb // 2), BF16),
            vm((seqs, width), F32),
            vm((2, n, outer * seqs, kb // 2), BF16),
            vm((outer, 2, 1, kb // 2), F32),
            vm((outer, 2, LANES, kb // 2), BF16),
            vm((tokens, kb // 2), F32),
            vm((tokens, LANES), F32),
            vm((tokens, 2 * cols + 2 * dcols + LANES), F32),
            vm((cols // tile, tokens, tile), BF16),
            vm((cols // tile, tokens, tile), BF16),
            vm((tokens, dcols), BF16),
            vm((tokens, dcols), BF16),
            vm((tokens, 2 * LANES), F32),
            vm((tokens, half), F32),
            vm((CHUNKS, INNER, outer, seqs, piece), BF16),
            vm((CHUNKS, outer, INNER, seqs, piece), BF16),
            vm((CHUNKS, outer, seqs, piece), BF16),
            vm((CHUNKS, outer, seqs, piece), BF16),
            vm((seqs, half), BF16),
            vm((seqs, half), BF16),
            sem((16,)),
            sem((n,)), sem((n,)), sem((2,)),
            sem((slabs, INNER)), sem((slabs, INNER)), sem((slabs + 1,)),
            sem((INNER,)), sem((2, span)),
            sem((n,)), sem((n,)),
            sem((slabs, n)), sem((slabs, n)),
            sem((slabs, 2 * outer)), sem((slabs, 2 * outer)),
            sem((outer,)), sem((outer,)),
            sem((outer,)), sem((outer, INNER)), sem((n,)),
            sem((n,)), sem((n,)),
            sem((cols // tile + 1,)), sem((cols // tile + 1,)),
            sem((CHUNKS, outer, INNER)), sem((CHUNKS, outer, INNER)),
            sem((CHUNKS, outer)), sem((CHUNKS, outer)),
            sem, sem, sem((2,)), sem((2,)),
        ],
        compiler_params=pltpu.CompilerParams(
            collective_id=0, has_side_effects=True, vmem_limit_bytes=56 * 2**20
        ),
        name="layer",
    )(*args)


def update_kernel(packed, state_ref, out_ref, new_ref):
    seqs, width = out_ref.shape
    heads, dim = state_ref.shape[1:3]
    hw = heads * dim
    tp = lax.axis_index("tp")
    out_ref[...] = packed[:, :width].astype(BF16)
    row = lax.broadcasted_iota(jnp.int32, (seqs, 2 * dim), 0)
    lane = lax.broadcasted_iota(jnp.int32, (seqs, 2 * dim), 1) // dim
    for h in range(heads):
        gamma = jnp.where(tp == 0, F32(decay(h, HEADS)), F32(decay(heads + h, HEADS)))
        key = packed[:, width + h * dim : width + (h + 1) * dim]
        key = split(key).T.astype(BF16)
        value = packed[:, width + hw + h * dim : width + hw + (h + 1) * dim]
        twice = jnp.concatenate([value, value], axis=1)
        for s in range(0, seqs, 2):
            spread = jnp.where(row == s + lane, twice, 0.0)
            spread = jnp.concatenate([spread] * PIECES, axis=0).astype(BF16)
            added = jnp.dot(key, spread, preferred_element_type=F32)
            for t in range(2):
                new_ref[s + t, h] = gamma * state_ref[s + t, h] + added[:, t * dim : (t + 1) * dim]


def update(packed, state):
    seqs, heads, dim = state.shape[:3]
    width = packed.shape[1] - 2 * heads * dim
    few = min(8, seqs)
    held = pl.BlockSpec((few, heads, dim, dim), lambda j: (j, 0, 0, 0))
    return pl.pallas_call(
        update_kernel,
        grid=(seqs // few,),
        out_shape=(
            jax.ShapeDtypeStruct((seqs, width), BF16),
            jax.ShapeDtypeStruct(state.shape, F32),
        ),
        in_specs=[pl.BlockSpec((few, packed.shape[1]), lambda j: (j, 0)), held],
        out_specs=(pl.BlockSpec((few, width), lambda j: (j, 0)), held),
        compiler_params=pltpu.CompilerParams(vmem_limit_bytes=16 * 2**20),
        name="update",
    )(packed, state)


def on_device(
    inputs,
    positions,
    ret_state,
    norm_mix,
    w_query,
    w_key,
    w_value,
    w_gate_in,
    head_gain,
    w_out,
    norm_ffn,
    route_ids,
    route_weight,
    exp_gate,
    exp_up,
    exp_down,
    dense_gate,
    dense_up,
    dense_down,
    branch_gate,
):
    n = lax.axis_size("ep")
    dim = ret_state.shape[2]
    assert exp_gate.shape[0] == 1 and n % (2 * INNER) == 0 and n <= LANES
    assert w_query.shape[1] % WIDE == 0 and WIDE % dim == 0
    turns = 10000.0 ** (-2.0 * np.arange(dim // 2) / dim)
    freq = jnp.asarray(np.concatenate([turns, turns])[None].astype(np.float32))
    packed = layer(
        n,
        (inputs, positions, freq, route_ids.T, route_weight.T, norm_mix, norm_ffn, branch_gate,
         head_gain, ret_state, w_query, w_key, w_value, w_gate_in, w_out, exp_gate, exp_up,
         exp_down, dense_gate, dense_up, dense_down),
    )
    return update(packed, ret_state)


def solution(mesh):
    in_specs = (
        P("ep", None),
        P("ep"),
        P("ep", "tp", None, None),
        P(),
        P("ep", "tp"),
        P("ep", "tp"),
        P("ep", "tp"),
        P("ep", "tp"),
        P("tp"),
        P("tp", "ep"),
        P(),
        P("ep", None),
        P("ep", None),
        P("ep", None, "tp"),
        P("ep", None, "tp"),
        P("ep", "tp", None),
        P(None, ("ep", "tp")),
        P(None, ("ep", "tp")),
        P(("ep", "tp"), None),
        P(),
    )
    out_specs = (P("ep", None), P("ep", "tp", None, None))
    return jax.shard_map(
        on_device, mesh=mesh, in_specs=in_specs, out_specs=out_specs, check_vma=False
    )
```
